32 devices in a mesh: fs: 16 (over z, y, x), tp: 2 (over core).
Axes of the slice: x: 2, y: 2, z: 4, core: 2. Of those that a mesh axis runs over, the one named last changes fastest.
Arguments:
- tokens: bfloat16 [6144, 2048], P('fs'), may hold values from -6 to 6
- merged: bfloat16 [6144, 2048], P('fs'), may hold values from -6 to 6
- gain_first: float32 [2048], replicated, may hold values from 0.1 to 1.9
- gate_first: bfloat16 [2048, 2816], P('fs', 'tp'), may hold values from -0.125 to 0.125
- up_first: bfloat16 [2048, 2816], P('fs', 'tp'), may hold values from -0.125 to 0.125
- down_first: bfloat16 [2816, 2048], P('tp', 'fs'), may hold values from -0.21875 to 0.21875
- gain_second: float32 [2048], replicated, may hold values from 0.1 to 1.9
- gate_second: bfloat16 [2048, 2816], P('fs', 'tp'), may hold values from -0.125 to 0.125
- up_second: bfloat16 [2048, 2816], P('fs', 'tp'), may hold values from -0.125 to 0.125
- down_second: bfloat16 [2816, 2048], P('tp', 'fs'), may hold values from -0.21875 to 0.21875
Outputs:
- result: bfloat16 [6144, 2048], P('fs')
The draws below stay inside these ranges and needn't reach their ends.
All inputs are finite; a program needn't handle non-finite values.
Results may differ from the reference program's by a relative error of at most 0.01.
Values may be sent and summed in bfloat16 or wider, within the bound.
A program may use at most 64 MiB of HBM per device.

```python
import jax
import jax.numpy as jnp
from jax import lax

D = 2048
FF = 2816
TOKENS = 6144
N_TP = 2


def level_of(key, dims, shards, least, largest):
    level = 1.0
    for axis_at, parts in shards:
        draws = jax.random.uniform(jax.random.fold_in(jax.random.fold_in(key, 6), axis_at), (parts,), jnp.float32, least / len(shards), largest / len(shards))
        level = level * jnp.repeat(jnp.exp(draws), dims[axis_at] // parts).reshape((-1,) + (1,) * (len(dims) - 1 - axis_at))
    return level


def scatter_about(rng, dims, deviation, most, split=(), held_as=jnp.bfloat16):
    result = jax.random.normal(rng, dims, jnp.float32) * deviation
    if len(split) > 0:
        result = level_of(rng, dims, split, -0.22, 0.18) * result
    return jnp.clip(result, min=-most, max=most).astype(held_as)


def setup_inputs(seed: int = 0) -> dict:
    seeds = jax.random.split(jax.random.key(seed), 11)
    tokens = scatter_about(seeds[0], (TOKENS, D), 1.0, 6.0, ((0, 16),))
    merged = scatter_about(seeds[1], (TOKENS, D), 1.0, 6.0, ((0, 16),))
    gain_first = jnp.clip(1.0 + 0.18 * jax.random.normal(seeds[2], (D,), jnp.float32), 0.1, 1.9)
    gate_first = scatter_about(seeds[3], (D, FF), D ** -0.5, 0.125, ((0, 16), (1, 2)))
    up_first = scatter_about(seeds[4], (D, FF), D ** -0.5, 0.125, ((0, 16), (1, 2)))
    down_first = scatter_about(seeds[5], (FF, D), (FF // 4) ** -0.5, 0.21875, ((0, 2), (1, 16)))
    gain_second = jnp.clip(1.0 + 0.18 * jax.random.normal(seeds[6], (D,), jnp.float32), 0.1, 1.9)
    gate_second = scatter_about(seeds[7], (D, FF), D ** -0.5, 0.125, ((0, 16), (1, 2)))
    up_second = scatter_about(seeds[8], (D, FF), D ** -0.5, 0.125, ((0, 16), (1, 2)))
    down_second = scatter_about(seeds[9], (FF, D), (FF // 4) ** -0.5, 0.21875, ((0, 2), (1, 16)))
    return {"tokens": tokens, "merged": merged, "gain_first": gain_first, "gate_first": gate_first, "up_first": up_first, "down_first": down_first, "gain_second": gain_second, "gate_second": gate_second, "up_second": up_second, "down_second": down_second}


EPS = 1e-06

def norm_rows(values, gain):
    scale = lax.rsqrt(lax.optimization_barrier(jnp.mean(values * values, axis=-1, keepdims=True)) + EPS)
    return values * scale * gain.astype(jnp.float32)

def half_step(normed, gate_weight, up_weight, down_weight):
    gate = jnp.dot(normed, gate_weight, preferred_element_type=jnp.float32)
    up = jnp.dot(normed, up_weight, preferred_element_type=jnp.float32)
    hidden = (jax.nn.silu(gate) * up).astype(jnp.bfloat16)
    width = FF // N_TP

    def add_block(index, total):
        start = (index * width).astype(jnp.int32)
        cols = lax.dynamic_slice_in_dim(hidden, start, width, 1)
        rows = lax.dynamic_slice_in_dim(down_weight, start, width, 0)
        part = jnp.dot(cols, rows, preferred_element_type=jnp.float32).astype(jnp.bfloat16)
        part = lax.optimization_barrier(part)
        return total + part.astype(jnp.float32)
    empty = jnp.zeros((normed.shape[0], down_weight.shape[1]), jnp.float32)
    return lax.fori_loop(0, N_TP, add_block, empty)

def reference(tokens, merged, gain_first, gate_first, up_first, down_first, gain_second, gate_second, up_second, down_second):
    source = tokens.astype(jnp.float32)
    normed_first = norm_rows(source, gain_first).astype(jnp.bfloat16)
    down_a = half_step(normed_first, gate_first, up_first, down_first)
    middle = source + merged.astype(jnp.float32) + 0.5 * down_a
    normed_second = norm_rows(middle, gain_second).astype(jnp.bfloat16)
    down_b = half_step(normed_second, gate_second, up_second, down_second)
    return (middle + 0.5 * down_b).astype(jnp.bfloat16)
```

```python
import functools

import jax
import jax.numpy as jnp
from jax import lax
from jax.experimental import pallas as pl
from jax.experimental.pallas import tpu as pltpu
from jax.sharding import PartitionSpec as P

EPS = 1e-06
BF16 = jnp.bfloat16
F32 = jnp.float32
PLANE = 4
LINE = 4


def norm_rows(values, gain):
    scale = lax.rsqrt(jnp.mean(values * values, axis=-1, keepdims=True) + EPS)
    return values * scale * gain


def gathered_block(normed, gate, up, down):
    gate_whole = lax.all_gather(gate, "fs", axis=0, tiled=True)
    up_whole = lax.all_gather(up, "fs", axis=0, tiled=True)
    g = jnp.dot(normed, gate_whole, preferred_element_type=F32)
    u = jnp.dot(normed, up_whole, preferred_element_type=F32)
    hidden = (jax.nn.silu(g) * u).astype(BF16)
    down_whole = lax.all_gather(down, "fs", axis=1, tiled=True)
    part = jnp.dot(hidden, down_whole, preferred_element_type=F32)
    return lax.psum(part.astype(BF16), "tp").astype(F32)


def gathered_shards(tokens, merged, gain1, g1, u1, d1, gain2, g2, u2, d2):
    source = tokens.astype(F32)
    middle = source + merged.astype(F32)
    normed = norm_rows(source, gain1).astype(BF16)
    middle = middle + 0.5 * gathered_block(normed, g1, u1, d1)
    normed = norm_rows(middle, gain2).astype(BF16)
    return (middle + 0.5 * gathered_block(normed, g2, u2, d2)).astype(BF16)


def kernel(
    tokens_h, merged_h, gain1, gain2, wa, wb, wc, wd, we, wf, out_h,
    raw, turned, straight, tokens, merged, out, w, normed1, normed2, acc_g, acc_u, hidden,
    part, own, sib, comb, diag, rsr, middle, ssq,
    load, p1_s, p1_r, z_s, z_r,
    ag_s, ag_r, rel_s, rel_r, sib_s, sib_r, rs_s, rs_r, fin_s, fin_r, store,
):
    weights_in = (wa, wb, wc, wd, we, wf)
    fs = lax.axis_index("fs")
    t = lax.axis_index("tp")
    z = fs // PLANE
    p = fs % PLANE
    rows, width = tokens.shape
    half = rows // 2
    quarter = half // 2
    q, pw = w.shape[1], width // LINE
    ds = wc.shape[1]
    step = 16

    def dev(zz, pp, tt):
        return {"fs": zz * PLANE + pp, "tp": tt}

    peers = (p, p + 1 - 2 * (p % 2), (p + 2) % PLANE, PLANE - 1 - p)
    to_peer = [dev(z, pp, t) for pp in peers]
    sibling = dev(z, p, 1 - t)

    low = (z < 2).astype(jnp.int32)
    toward = 2 * low - 1
    mid = (z % 3 != 0).astype(jnp.int32)
    zi, zo = z + toward, z - toward * mid
    inner, outer = dev(zi, p, t), dev(zo, p, t)

    def on_mid(f):
        pl.when(mid == 1)(f)

    def on_end(f):
        pl.when(mid == 0)(f)

    def remote(src, dst, s, r, to):
        return pltpu.make_async_remote_copy(
            src_ref=src, dst_ref=dst, send_sem=s, recv_sem=r,
            device_id=to, device_id_type=pl.DeviceIdType.MESH,
        )

    mine = pl.ds(pl.multiple_of(t * half, 16), half)
    other = pl.ds(pl.multiple_of((1 - t) * half, 16), half)

    def shard_of(m):
        k = m // 3
        return straight.at[k] if m % 3 == 2 else turned.at[2 * k + m % 3]

    def loading(m):
        k = m // 3
        return pltpu.make_async_copy(
            weights_in[m], straight.at[k] if m % 3 == 2 else raw.at[2 * k + m % 3], load.at[m]
        )

    load_tokens = pltpu.make_async_copy(tokens_h, tokens, load.at[6])
    load_merged = pltpu.make_async_copy(merged_h, merged, load.at[7])
    loading(0).start()
    loading(1).start()
    load_tokens.start()
    for m in (2, 3, 4, 5):
        loading(m).start()
    load_merged.start()

    barrier = pltpu.get_barrier_semaphore()
    targets = [inner, sibling] + to_peer[1:]
    for to in targets:
        pl.semaphore_signal(barrier, inc=1, device_id=to, device_id_type=pl.DeviceIdType.MESH)

    @on_mid
    def _():
        pl.semaphore_signal(barrier, inc=1, device_id=outer, device_id_type=pl.DeviceIdType.MESH)

    def turn(m):
        k = 2 * (m // 3) + m % 3
        loading(m).wait()
        for j in range(raw.shape[2] // 128):
            turned[k, j * 128:(j + 1) * 128, :] = raw[k, :, j * 128:(j + 1) * 128].T

    def lanes_of(zz, pp):
        return pl.ds(pl.multiple_of((zz * PLANE + pp) * ds, ds), ds)

    def p1(m, r):
        src = shard_of(m).at[pl.ds(pl.multiple_of(peers[r] * q, 16), q), :]
        return remote(src, w.at[m, :, lanes_of(z, p)], p1_s.at[m, r - 1], p1_r.at[m, r - 1], to_peer[r])

    def p1_in(m, r):
        src = w.at[m, :, lanes_of(z, peers[r])]
        return remote(src, src, p1_s.at[m, r - 1], p1_r.at[m, r - 1], to_peer[r])

    def start_p1(m):
        for r in (3, 1, 2):
            p1(m, r).start()
        w[m, :, lanes_of(z, p)] = shard_of(m)[pl.ds(pl.multiple_of(p * q, 16), q), :]

    def blk(m, zz):
        return w.at[m, :, pl.ds(pl.multiple_of(zz * pw, pw), pw)]

    first_slot = 3 * (1 - mid)

    def to_inner(m, r=None):
        at = blk(m, z) if r is None else w.at[m, :, lanes_of(z, peers[r])]
        return remote(at, at, z_s.at[m, 0], z_r.at[m, first_slot], inner)

    def to_outer(m, r=None):
        at = blk(m, z) if r is None else w.at[m, :, lanes_of(z, peers[r])]
        return remote(at, at, z_s.at[m, 1], z_r.at[m, 0], outer)

    def on_inner(m):
        return remote(blk(m, zo), blk(m, zo), z_s.at[m, 2], z_r.at[m, 1], inner)

    def on_outer(m, d):
        at = blk(m, z + d * toward)
        return remote(at, at, z_s.at[m, 2 + d], z_r.at[m, d], outer)

    def came(m, slot):
        zz = zo if slot == 3 else z + (slot + 1) * toward
        return remote(blk(m, zz), blk(m, zz), z_s.at[m, 0], z_r.at[m, slot], inner)

    def piece_out(m, r):
        to_inner(m, r).start()

        @on_mid
        def _():
            to_outer(m, r).start()

    def own_now(m):
        for r in (1, 2, 3):
            p1_in(m, r).wait_recv()
            piece_out(m, r)

    def own_inner(m):
        for r in (1, 2, 3):
            p1_in(m, r).wait_recv()
        to_inner(m).start()

    def own_outer(m):
        @on_mid
        def _():
            to_outer(m).start()

    def pass_in(m):
        @on_mid
        def _():
            came(m, 3).wait_recv()
            on_inner(m).start()

    def pass_out(m, d):
        @on_mid
        def _():
            came(m, d - 1).wait_recv()
            on_outer(m, d).start()

    def need(m, slot):
        @on_end
        def _():
            came(m, slot).wait_recv()

    bufs = (normed1, normed2)

    def piece(tt, h):
        return pl.ds(pl.multiple_of(tt * half + h * quarter, 16), quarter)

    def ag(f, r, h):
        at = piece(t, h)
        return remote(bufs[f].at[0, at, :], bufs[f].at[r, at, :], ag_s.at[f, r - 1, h], ag_r.at[f, r - 1, h], to_peer[r])

    def ag_on(f, h):
        at = piece(t, h)
        return remote(bufs[f].at[2 - h, at, :], bufs[f].at[3, at, :], ag_s.at[f, 2, h], ag_r.at[f, 2, h], to_peer[1 + h])

    def relay(f, r, h, tt):
        at = bufs[f].at[r, piece(tt, h), :]
        return remote(at, at, rel_s.at[f, r, h], rel_r.at[f, r, h], sibling)

    def ag_first(f):
        for r, h in ((2, 0), (1, 1)):
            ag(f, r, h).wait_recv()
            ag_on(f, h).start()
            relay(f, r, h, t).start()

    def ag_second(f):
        for r, h in ((2, 1), (1, 0)):
            ag(f, r, h).wait_recv()
            relay(f, r, h, t).start()

    def ag_far(f):
        for h in range(2):
            ag_on(f, h).wait_recv()
            relay(f, 3, h, t).start()

    zs = (z, zi, jnp.where(mid == 1, zo, z + 2 * toward), jnp.where(mid == 1, z + 2 * toward, z + 3 * toward))
    lanes = [pl.ds(pl.multiple_of(zz * pw, pw), pw) for zz in zs]
    lanes_a = pl.ds(pl.multiple_of((1 - low) * pw, pw), 3 * pw)
    lanes_b = pl.ds(pl.multiple_of(low * 3 * pw, pw), pw)
    first, second = pl.ds(0, quarter), pl.ds(quarter, quarter)

    def to_sibling(f, c, r):
        return remote(part.at[r, :, lanes[c]], sib.at[r, :, lanes[c]], sib_s.at[f, c, r], sib_r.at[f, c, r], sibling)

    def rs(f, c, kind):
        at = lanes[c]
        src, dst, r = (
            (comb.at[2, first, at], diag.at[0, :, at], 1),
            (comb.at[2, second, at], diag.at[1, :, at], 2),
            (comb.at[0, first, at], rsr.at[0, first, at], 1),
            (comb.at[0, second, at], rsr.at[0, second, at], 1),
            (comb.at[1, second, at], rsr.at[1, second, at], 2),
            (comb.at[1, first, at], rsr.at[1, first, at], 2),
        )[kind]
        return remote(src, dst, rs_s.at[f, c, kind], rs_r.at[f, c, kind], to_peer[r])

    def product(f, k, r, at):
        dims = (((1,), (1,)), ((), ()))
        return lax.dot_general(bufs[f][r, :, at], w[3 * f + k, :, at], dims, preferred_element_type=F32)

    def gate_start(f):
        @pl.loop(0, PLANE)
        def _(r):
            @pl.when(r > (0 if f == 0 else -1))
            def _():
                for h in range(2):
                    relay(f, r, h, 1 - t).wait_recv()

            acc_g[r] = product(f, 0, r, lanes_a)

    def up_start(f):
        @pl.loop(0, PLANE)
        def _(r):
            acc_u[r] = product(f, 1, r, lanes_a)

    def gate_end(f):
        @pl.loop(0, PLANE)
        def _(r):
            g = acc_g[r] + product(f, 0, r, lanes_b)
            acc_g[r] = g / (1.0 + jnp.exp(-g))

    def up_end(f):
        @pl.loop(0, PLANE)
        def _(r):
            u = acc_u[r] + product(f, 1, r, lanes_b)
            hidden[r] = (acc_g[r] * u).astype(BF16)

    def down(f, c):
        at = lanes[c]

        @pl.loop(0, PLANE)
        def _(k):
            r = PLANE - 1 - k
            part[r, :, at] = jnp.dot(hidden[r, other, :], w[3 * f + 2, :, at], preferred_element_type=F32).astype(BF16)
            to_sibling(f, c, r).start()
            own[r, :, at] = jnp.dot(hidden[r, mine, :], w[3 * f + 2, :, at], preferred_element_type=F32).astype(BF16)

        for r, kinds in ((3, (0, 1)), (1, (2,)), (2, (4,))):
            to_sibling(f, c, r).wait_recv()

            @pl.loop(0, half // (2 * step))
            def _(i):
                some = pl.ds(pl.multiple_of(i * 2 * step, step), 2 * step)
                comb[r - 1, some, at] = (own[r, some, at].astype(F32) + sib[r, some, at].astype(F32)).astype(BF16)

            for kind in kinds:
                rs(f, c, kind).start()
        to_sibling(f, c, 0).wait_recv()

    def finish(f, c):
        at = lanes[c]
        rs(f, c, 0).wait_recv()
        comb[1, first, at] = (comb[1, first, at].astype(F32) + diag[0, :, at].astype(F32)).astype(BF16)
        rs(f, c, 5).start()
        rs(f, c, 1).wait_recv()
        comb[0, second, at] = (comb[0, second, at].astype(F32) + diag[1, :, at].astype(F32)).astype(BF16)
        rs(f, c, 3).start()

    def reduced(rows_at, at):
        total = own[0, rows_at, at].astype(F32) + sib[0, rows_at, at].astype(F32)
        return total + rsr[0, rows_at, at].astype(F32) + rsr[1, rows_at, at].astype(F32)

    def out_across(c):
        return remote(out.at[mine, lanes[c]], out.at[mine, lanes[c]], fin_s.at[c], fin_r.at[c], sibling)

    def out_here(c, at):
        k = 0 if at is mine else 1
        return pltpu.make_async_copy(out.at[at, lanes[c]], out_h.at[at, lanes[c]], store.at[k, c])

    def land(f, c):
        for kind in (2, 4, 3, 5):
            rs(f, c, kind).wait_recv()
        at = lanes[c]

        @pl.loop(0, half // (2 * step))
        def _(i):
            some = pl.ds(pl.multiple_of(i * 2 * step, step), 2 * step)
            full = pl.ds(pl.multiple_of(t * half + i * 2 * step, step), 2 * step)
            if f == 0:
                value = tokens[full, at].astype(F32) + merged[full, at].astype(F32) + 0.5 * reduced(some, at)
                middle[some, at] = value
                squares = value * value
                sums = sum(squares[:, k * 128:(k + 1) * 128] for k in range(pw // 128))
                ssq[some, :] = sums if c == 0 else ssq[some, :] + sums
            else:
                out[full, at] = (middle[some, at] + 0.5 * reduced(some, at)).astype(BF16)

        if f == 1:
            out_across(c).start()
            out_here(c, mine).start()

    def norm_first(start, count):
        @pl.loop(0, count // step)
        def _(i):
            at = pl.ds(pl.multiple_of(start + i * step, step), step)
            normed1[0, at, :] = norm_rows(tokens[at, :].astype(F32), gain1[...]).astype(BF16)

    turn(0)
    pl.semaphore_wait(barrier, len(targets) + mid)
    start_p1(0)
    piece_out(0, 0)
    turn(1)
    start_p1(1)
    piece_out(1, 0)

    load_tokens.wait()
    for h in range(2):
        norm_first(t * half + h * quarter, quarter)
        ag(0, 2 - h, h).start()
        ag(0, 1 + h, h).start()
    loading(2).wait()
    start_p1(2)
    own_now(0)
    norm_first((1 - t) * half, half)
    own_now(1)
    turn(3)
    turn(4)
    pass_in(0)
    pass_out(0, 1)
    ag_first(0)
    loading(5).wait()
    for m in (3, 4, 5):
        start_p1(m)
    pass_in(1)
    pass_out(1, 1)
    ag_second(0)
    pass_out(0, 2)
    own_inner(2)
    pass_out(1, 2)
    own_outer(2)
    ag_far(0)

    for slot in (0, 1):
        need(0, slot)
    gate_start(0)
    for slot in (0, 1):
        need(1, slot)
    up_start(0)
    pass_in(2)
    pass_out(2, 1)
    need(0, 2)
    gate_end(0)
    need(1, 2)
    up_end(0)
    down(0, 0)
    own_inner(3)
    need(2, 0)
    down(0, 1)
    finish(0, 0)
    need(2, 1)
    down(0, 2)
    finish(0, 1)
    pass_out(2, 2)
    own_outer(3)
    own_inner(4)
    own_inner(5)
    load_merged.wait()
    land(0, 0)
    need(2, 2)
    down(0, 3)
    finish(0, 2)
    land(0, 1)
    pass_in(3)
    pass_out(3, 1)
    finish(0, 3)
    land(0, 2)
    land(0, 3)

    for h in range(2):
        @pl.loop(0, quarter // step)
        def _(i):
            at = pl.ds(pl.multiple_of(h * quarter + i * step, step), step)
            full = pl.ds(pl.multiple_of(t * half + h * quarter + i * step, step), step)
            scale = lax.rsqrt(jnp.sum(ssq[at, :], axis=-1, keepdims=True) / width + EPS)
            normed2[0, full, :] = (middle[at, :] * scale * gain2[...]).astype(BF16)

        ag(1, 2 - h, h).start()
        ag(1, 1 + h, h).start()
        relay(1, 0, h, t).start()

    pass_out(3, 2)
    own_outer(4)
    pass_in(4)
    pass_out(4, 1)
    ag_first(1)
    pass_out(4, 2)
    own_outer(5)
    pass_in(5)
    pass_out(5, 1)
    ag_second(1)
    pass_out(5, 2)
    ag_far(1)

    for slot in (0, 1):
        need(3, slot)
    gate_start(1)
    for slot in (0, 1):
        need(4, slot)
    up_start(1)
    need(3, 2)
    gate_end(1)
    need(4, 2)
    up_end(1)
    for c in range(LINE):
        for r in range(PLANE):
            to_sibling(0, c, r).wait_send()
        for kind in range(6):
            rs(0, c, kind).wait_send()
    down(1, 0)
    need(5, 0)
    down(1, 1)
    finish(1, 0)
    need(5, 1)
    down(1, 2)
    finish(1, 1)
    land(1, 0)
    need(5, 2)
    down(1, 3)
    finish(1, 2)
    land(1, 1)
    finish(1, 3)
    land(1, 2)
    land(1, 3)

    for m in range(6):
        for r in (1, 2, 3):
            p1(m, r).wait_send()
        to_inner(m).wait_send()

        @on_mid
        def _():
            to_outer(m).wait_send()
            on_inner(m).wait_send()
            on_outer(m, 1).wait_send()
            on_outer(m, 2).wait_send()

    for f in range(2):
        for h in range(2):
            for r in (1, 2):
                ag(f, r, h).wait_send()
            ag_on(f, h).wait_send()
            for r in range(1 - f, PLANE):
                relay(f, r, h, t).wait_send()
    for c in range(LINE):
        for r in range(PLANE):
            to_sibling(1, c, r).wait_send()
        for kind in range(6):
            rs(1, c, kind).wait_send()
    theirs = [remote(out.at[other, lanes[c]], out.at[other, lanes[c]], fin_s.at[c], fin_r.at[c], sibling) for c in range(LINE)]
    for c in range(LINE):
        theirs[c].wait_recv()
        out_here(c, other).start()
    for c in range(LINE):
        out_across(c).wait_send()
        out_here(c, mine).wait()
        out_here(c, other).wait()


def plane_shards(tokens, merged, gain1, g1, u1, d1, gain2, g2, u2, d2):
    rows, width = tokens.shape
    half = rows // 2
    hid, ds = d1.shape
    q = hid // PLANE
    vmem = pl.BlockSpec(memory_space=pltpu.VMEM)
    far = pl.BlockSpec(memory_space=pl.ANY)
    dma = lambda *s: pltpu.SemaphoreType.DMA(s)
    return pl.pallas_call(
        kernel,
        out_shape=jax.ShapeDtypeStruct((rows, width), BF16),
        in_specs=[far, far, vmem, vmem] + [far] * 6,
        out_specs=far,
        scratch_shapes=[
            pltpu.VMEM((4, ds, hid), BF16),
            pltpu.VMEM((4, hid, ds), BF16),
            pltpu.VMEM((2, hid, ds), BF16),
            pltpu.VMEM((rows, width), BF16),
            pltpu.VMEM((rows, width), BF16),
            pltpu.VMEM((rows, width), BF16),
            pltpu.VMEM((6, q, width), BF16),
            pltpu.VMEM((PLANE, rows, width), BF16),
            pltpu.VMEM((PLANE, rows, width), BF16),
            pltpu.VMEM((PLANE, rows, q), F32),
            pltpu.VMEM((PLANE, rows, q), F32),
            pltpu.VMEM((PLANE, rows, q), BF16),
            pltpu.VMEM((PLANE, half, width), BF16),
            pltpu.VMEM((PLANE, half, width), BF16),
            pltpu.VMEM((PLANE, half, width), BF16),
            pltpu.VMEM((PLANE - 1, half, width), BF16),
            pltpu.VMEM((2, half // 2, width), BF16),
            pltpu.VMEM((2, half, width), BF16),
            pltpu.VMEM((half, width), F32),
            pltpu.VMEM((half, 128), F32),
            dma(8), dma(6, 3), dma(6, 3), dma(6, 5), dma(6, 4),
            dma(2, 3, 2), dma(2, 3, 2), dma(2, 4, 2), dma(2, 4, 2),
            dma(2, LINE, 4), dma(2, LINE, 4), dma(2, LINE, 6), dma(2, LINE, 6),
            dma(LINE), dma(LINE), dma(2, LINE),
        ],
        compiler_params=pltpu.CompilerParams(
            collective_id=0, has_side_effects=True, vmem_limit_bytes=60 * 2**20
        ),
    )(tokens, merged, gain1[None], gain2[None], g1, u1, d1, g2, u2, d2)


def shards(n_fs, n_tp, *args):
    rows, width = args[0].shape
    hid, cols = args[5].shape
    fits = n_fs == PLANE * LINE and n_tp == 2 and cols % 128 == 0
    fits = fits and hid % (32 * PLANE) == 0 and rows % 64 == 0
    return plane_shards(*args) if fits else gathered_shards(*args)


def solution(mesh):
    return jax.shard_map(
        functools.partial(shards, mesh.shape["fs"], mesh.shape["tp"]),
        mesh=mesh,
        in_specs=(
            P("fs", None),
            P("fs", None),
            P(),
            P("fs", "tp"),
            P("fs", "tp"),
            P("tp", "fs"),
            P(),
            P("fs", "tp"),
            P("fs", "tp"),
            P("tp", "fs"),
        ),
        out_specs=P("fs", None),
        check_vma=False,
    )
```

```python
import functools

import jax
import jax.numpy as jnp
from jax import lax
from jax.experimental import pallas as pl
from jax.experimental.pallas import tpu as pltpu
from jax.sharding import PartitionSpec as P

EPS = 1e-06
BF16 = jnp.bfloat16
F32 = jnp.float32
PLANE = 4
LINE = 4


def norm_rows(values, gain):
    scale = lax.rsqrt(jnp.mean(values * values, axis=-1, keepdims=True) + EPS)
    return values * scale * gain


def gathered_block(normed, gate, up, down):
    gate_whole = lax.all_gather(gate, "fs", axis=0, tiled=True)
    up_whole = lax.all_gather(up, "fs", axis=0, tiled=True)
    g = jnp.dot(normed, gate_whole, preferred_element_type=F32)
    u = jnp.dot(normed, up_whole, preferred_element_type=F32)
    hidden = (jax.nn.silu(g) * u).astype(BF16)
    down_whole = lax.all_gather(down, "fs", axis=1, tiled=True)
    part = jnp.dot(hidden, down_whole, preferred_element_type=F32)
    return lax.psum(part.astype(BF16), "tp").astype(F32)


def gathered_shards(tokens, merged, gain1, g1, u1, d1, gain2, g2, u2, d2):
    source = tokens.astype(F32)
    middle = source + merged.astype(F32)
    normed = norm_rows(source, gain1).astype(BF16)
    middle = middle + 0.5 * gathered_block(normed, g1, u1, d1)
    normed = norm_rows(middle, gain2).astype(BF16)
    return (middle + 0.5 * gathered_block(normed, g2, u2, d2)).astype(BF16)


def kernel(
    tokens_h, merged_h, gain1_h, gain2_h, wa, wb, wc, wd, we, wf, out,
    raw, turned, straight, tokens, merged, gain1, gain2, fin, w, normed1, normed2, acc_g, acc_u, hidden,
    part, own, sib, comb, diag, rsr, middle, ssq,
    load, p1_s, p1_r, z_s, z_r,
    ag_s, ag_r, rel_s, rel_r, sib_s, sib_r, rs_s, rs_r, fin_s, fin_r,
):
    weights_in = (wa, wb, wc, wd, we, wf)
    fs = lax.axis_index("fs")
    t = lax.axis_index("tp")
    z = fs // PLANE
    p = fs % PLANE
    rows, width = tokens.shape
    half = rows // 2
    quarter = half // 2
    q, pw = w.shape[1], width // LINE
    ds = wc.shape[1]
    step = 16

    def dev(zz, pp, tt):
        return {"fs": zz * PLANE + pp, "tp": tt}

    peers = (p, p + 1 - 2 * (p % 2), (p + 2) % PLANE, PLANE - 1 - p)
    to_peer = [dev(z, pp, t) for pp in peers]
    sibling = dev(z, p, 1 - t)

    low = (z < 2).astype(jnp.int32)
    toward = 2 * low - 1
    mid = (z % 3 != 0).astype(jnp.int32)
    zi, zo = z + toward, z - toward * mid
    inner, outer = dev(zi, p, t), dev(zo, p, t)

    def on_mid(f):
        pl.when(mid == 1)(f)

    def on_end(f):
        pl.when(mid == 0)(f)

    def remote(src, dst, s, r, to):
        return pltpu.make_async_remote_copy(
            src_ref=src, dst_ref=dst, send_sem=s, recv_sem=r,
            device_id=to, device_id_type=pl.DeviceIdType.MESH,
        )

    mine = pl.ds(pl.multiple_of(t * half, 16), half)
    other = pl.ds(pl.multiple_of((1 - t) * half, 16), half)

    def shard_of(m):
        k = m // 3
        return straight.at[k] if m % 3 == 2 else turned.at[2 * k + m % 3]

    def loading(m):
        k = m // 3
        return pltpu.make_async_copy(
            weights_in[m], straight.at[k] if m % 3 == 2 else raw.at[2 * k + m % 3], load.at[m]
        )

    load_tokens = pltpu.make_async_copy(tokens_h, tokens, load.at[6])
    load_merged = pltpu.make_async_copy(merged_h, merged, load.at[7])
    load_gain1 = pltpu.make_async_copy(gain1_h, gain1, load.at[8])
    load_gain2 = pltpu.make_async_copy(gain2_h, gain2, load.at[9])
    for m in (2, 0, 1):
        loading(m).start()
    load_tokens.start()
    load_gain1.start()
    for m in (5, 3, 4):
        loading(m).start()
    load_merged.start()
    load_gain2.start()

    barrier = pltpu.get_barrier_semaphore()
    targets = [inner, sibling] + to_peer[1:]
    for to in targets:
        pl.semaphore_signal(barrier, inc=1, device_id=to, device_id_type=pl.DeviceIdType.MESH)

    @on_mid
    def _():
        pl.semaphore_signal(barrier, inc=1, device_id=outer, device_id_type=pl.DeviceIdType.MESH)

    def turn(m):
        k = 2 * (m // 3) + m % 3
        loading(m).wait()
        for j in range(raw.shape[2] // 128):
            turned[k, j * 128:(j + 1) * 128, :] = raw[k, :, j * 128:(j + 1) * 128].T

    def lanes_of(zz, pp):
        return pl.ds(pl.multiple_of((zz * PLANE + pp) * ds, ds), ds)

    def p1(m, r):
        src = shard_of(m).at[pl.ds(pl.multiple_of(peers[r] * q, 16), q), :]
        return remote(src, w.at[m, :, lanes_of(z, p)], p1_s.at[m, r - 1], p1_r.at[m, r - 1], to_peer[r])

    def p1_in(m, r):
        src = w.at[m, :, lanes_of(z, peers[r])]
        return remote(src, src, p1_s.at[m, r - 1], p1_r.at[m, r - 1], to_peer[r])

    def place(m):
        w[m, :, lanes_of(z, p)] = shard_of(m)[pl.ds(pl.multiple_of(p * q, 16), q), :]

    def start_p1(m):
        for r in (3, 1, 2):
            p1(m, r).start()

    def blk(m, zz):
        return w.at[m, :, pl.ds(pl.multiple_of(zz * pw, pw), pw)]

    first_slot = 3 * (1 - mid)

    def to_inner(m, r=None):
        at = blk(m, z) if r is None else w.at[m, :, lanes_of(z, peers[r])]
        return remote(at, at, z_s.at[m, 0], z_r.at[m, first_slot], inner)

    def to_outer(m, r=None):
        at = blk(m, z) if r is None else w.at[m, :, lanes_of(z, peers[r])]
        return remote(at, at, z_s.at[m, 1], z_r.at[m, 0], outer)

    def on_inner(m):
        return remote(blk(m, zo), blk(m, zo), z_s.at[m, 2], z_r.at[m, 1], inner)

    def on_outer(m, d):
        at = blk(m, z + d * toward)
        return remote(at, at, z_s.at[m, 2 + d], z_r.at[m, d], outer)

    def last_half(k):
        at = w.at[5, :, pl.ds(pl.multiple_of((z + (3 - mid) * toward) * pw + k * pw // 2, pw // 2), pw // 2)]
        return remote(at, at, z_s.at[5, 4 + k], z_r.at[5, (2, 4)[k]], outer)

    def came(m, slot):
        zz = zo if slot == 3 else z + (slot + 1) * toward
        return remote(blk(m, zz), blk(m, zz), z_s.at[m, 0], z_r.at[m, slot], inner)

    def piece_out(m, r):
        to_inner(m, r).start()

        @on_mid
        def _():
            to_outer(m, r).start()

    def own_now(m):
        for r in (1, 2, 3):
            p1_in(m, r).wait_recv()
            piece_out(m, r)

    def own_inner(m, begun=False):
        for r in (1, 2, 3):
            p1_in(m, r).wait_recv()
            if begun:
                to_inner(m, r).start()
        if not begun:
            to_inner(m).start()

    def own_outer(m, begun=False):
        @on_mid
        def _():
            if begun:
                for r in (1, 2, 3):
                    to_outer(m, r).start()
            else:
                to_outer(m).start()

    def pass_in(m):
        @on_mid
        def _():
            came(m, 3).wait_recv()
            on_inner(m).start()

    def pass_out(m, d):
        @on_mid
        def _():
            came(m, d - 1).wait_recv()
            on_outer(m, d).start()

    def need(m, slot):
        @on_end
        def _():
            came(m, slot).wait_recv()

    bufs = (normed1, normed2)

    def piece(tt, h):
        return pl.ds(pl.multiple_of(tt * half + h * quarter, 16), quarter)

    def ag(f, r, h):
        at = piece(t, h)
        return remote(bufs[f].at[0, at, :], bufs[f].at[r, at, :], ag_s.at[f, r - 1, h], ag_r.at[f, r - 1, h], to_peer[r])

    def ag_on(f, h):
        at = piece(t, h)
        return remote(bufs[f].at[2 - h, at, :], bufs[f].at[3, at, :], ag_s.at[f, 2, h], ag_r.at[f, 2, h], to_peer[1 + h])

    def relay(f, r, h, tt):
        at = bufs[f].at[r, piece(tt, h), :]
        return remote(at, at, rel_s.at[f, r, h], rel_r.at[f, r, h], sibling)

    def ag_first(f):
        for r, h in ((2, 0), (1, 1)):
            ag(f, r, h).wait_recv()
            ag_on(f, h).start()
            relay(f, r, h, t).start()

    def ag_second(f):
        for r, h in ((2, 1), (1, 0)):
            ag(f, r, h).wait_recv()
            relay(f, r, h, t).start()

    def ag_far(f):
        for h in range(2):
            ag_on(f, h).wait_recv()
            relay(f, 3, h, t).start()

    def need_half(k):
        @on_end
        def _():
            last_half(k).wait_recv()

    zs = (z, zi, jnp.where(mid == 1, zo, z + 2 * toward), jnp.where(mid == 1, z + 2 * toward, z + 3 * toward))
    hw = pw // 2
    widths = ((pw,) * LINE, (pw,) * (LINE - 1) + (hw, hw))
    lanes = [[pl.ds(pl.multiple_of(zz * pw, pw), pw) for zz in zs]]
    lanes.append(lanes[0][:-1] + [pl.ds(pl.multiple_of(zs[-1] * pw + k * hw, hw), hw) for k in range(2)])
    lanes_a = pl.ds(pl.multiple_of((1 - low) * pw, pw), 3 * pw)
    lanes_b = pl.ds(pl.multiple_of(low * 3 * pw, pw), pw)
    first, second = pl.ds(0, quarter), pl.ds(quarter, quarter)

    def to_sibling(f, c, r):
        return remote(part.at[r, :, lanes[f][c]], sib.at[r, :, lanes[f][c]], sib_s.at[f, c, r], sib_r.at[f, c, r], sibling)

    def rs(f, c, kind):
        at = lanes[f][c]
        src, dst, r = (
            (comb.at[2, first, at], diag.at[0, :, at], 1),
            (comb.at[2, second, at], diag.at[1, :, at], 2),
            (comb.at[0, first, at], rsr.at[0, first, at], 1),
            (comb.at[0, second, at], rsr.at[0, second, at], 1),
            (comb.at[1, second, at], rsr.at[1, second, at], 2),
            (comb.at[1, first, at], rsr.at[1, first, at], 2),
        )[kind]
        return remote(src, dst, rs_s.at[f, c, kind], rs_r.at[f, c, kind], to_peer[r])

    def product(f, k, r, at):
        dims = (((1,), (1,)), ((), ()))
        return lax.dot_general(bufs[f][r, :, at], w[3 * f + k, :, at], dims, preferred_element_type=F32)

    def slot_in(f, r):
        @pl.when(r > (0 if f == 0 else -1))
        def _():
            for h in range(2):
                relay(f, r, h, 1 - t).wait_recv()

    def silu(g):
        return g / (1.0 + jnp.exp(-g))

    def make_hidden(f):
        every = slice(None)

        @on_mid
        def _():
            @pl.loop(0, PLANE)
            def _(r):
                slot_in(f, r)
                g = silu(product(f, 0, r, every))
                hidden[r] = (g * product(f, 1, r, every)).astype(BF16)

        @on_end
        def _():
            for m, slot in ((0, 0), (0, 1), (0, 2), (1, 0), (1, 1)):
                came(3 * f + m, slot).wait_recv()

            @pl.loop(0, PLANE)
            def _(r):
                slot_in(f, r)
                acc_g[r] = silu(product(f, 0, r, every))
                acc_u[r] = product(f, 1, r, lanes_a)

            came(3 * f + 1, 2).wait_recv()

            @pl.loop(0, PLANE)
            def _(r):
                u = acc_u[r] + product(f, 1, r, lanes_b)
                hidden[r] = (acc_g[r] * u).astype(BF16)

    def down(f, c):
        at = lanes[f][c]

        def part_of(r, rows_at):
            return jnp.dot(hidden[r, rows_at, :], w[3 * f + 2, :, at], preferred_element_type=F32).astype(BF16)

        @pl.loop(0, PLANE)
        def _(k):
            r = PLANE - 1 - k
            part[r, :, at] = part_of(r, other)
            to_sibling(f, c, r).start()

        for r, kinds in ((3, (0, 1)), (2, (4,)), (1, (2,))):
            own[r, :, at] = part_of(r, mine)
            to_sibling(f, c, r).wait_recv()

            @pl.loop(0, half // (2 * step))
            def _(i):
                some = pl.ds(pl.multiple_of(i * 2 * step, step), 2 * step)
                comb[r - 1, some, at] = (own[r, some, at].astype(F32) + sib[r, some, at].astype(F32)).astype(BF16)

            for kind in kinds:
                rs(f, c, kind).start()
        own[0, :, at] = part_of(0, mine)
        to_sibling(f, c, 0).wait_recv()

    def finish(f, c):
        at = lanes[f][c]
        rs(f, c, 0).wait_recv()
        comb[1, first, at] = (comb[1, first, at].astype(F32) + diag[0, :, at].astype(F32)).astype(BF16)
        rs(f, c, 5).start()
        rs(f, c, 1).wait_recv()
        comb[0, second, at] = (comb[0, second, at].astype(F32) + diag[1, :, at].astype(F32)).astype(BF16)
        rs(f, c, 3).start()

    def reduced(rows_at, at):
        total = own[0, rows_at, at].astype(F32) + sib[0, rows_at, at].astype(F32)
        return total + rsr[0, rows_at, at].astype(F32) + rsr[1, rows_at, at].astype(F32)

    def out_across(c):
        at = lanes[1][c]
        return remote(out.at[mine, at], fin.at[:, at], fin_s.at[c], fin_r.at[c], sibling)

    def land(f, c):
        for kind in (2, 4, 3, 5):
            rs(f, c, kind).wait_recv()
        at = lanes[f][c]

        @pl.loop(0, half // (2 * step))
        def _(i):
            some = pl.ds(pl.multiple_of(i * 2 * step, step), 2 * step)
            full = pl.ds(pl.multiple_of(t * half + i * 2 * step, step), 2 * step)
            if f == 0:
                value = tokens[full, at].astype(F32) + merged[full, at].astype(F32) + 0.5 * reduced(some, at)
                middle[some, at] = value
                squares = value * value
                sums = sum(squares[:, k * 128:(k + 1) * 128] for k in range(widths[f][c] // 128))
                ssq[some, :] = sums if c == 0 else ssq[some, :] + sums
            else:
                out[full, at] = (middle[some, at] + 0.5 * reduced(some, at)).astype(BF16)

        if f == 1:
            out_across(c).start()

    def norm_first(start, count):
        @pl.loop(0, count // step)
        def _(i):
            at = pl.ds(pl.multiple_of(start + i * step, step), step)
            normed1[0, at, :] = norm_rows(tokens[at, :].astype(F32), gain1[...]).astype(BF16)

    loading(2).wait()
    place(2)
    pl.semaphore_wait(barrier, len(targets) + mid)
    piece_out(2, 0)
    turn(0)
    start_p1(0)
    place(0)
    piece_out(0, 0)
    turn(1)
    start_p1(1)
    place(1)
    piece_out(1, 0)
    loading(5).wait()
    place(5)
    piece_out(5, 0)

    load_tokens.wait()
    load_gain1.wait()
    for h in range(2):
        norm_first(t * half + h * quarter, quarter)
        ag(0, 2 - h, h).start()
        ag(0, 1 + h, h).start()
    start_p1(2)
    own_now(0)
    norm_first((1 - t) * half, half)
    own_now(1)
    turn(3)
    turn(4)
    pass_in(0)
    pass_out(0, 1)
    ag_first(0)
    for m in (3, 4, 5):
        start_p1(m)
    place(3)
    place(4)
    pass_in(1)
    pass_out(1, 1)
    ag_second(0)
    pass_out(0, 2)
    own_inner(2, True)
    pass_out(1, 2)
    own_outer(2, True)
    ag_far(0)

    make_hidden(0)
    pass_in(2)
    pass_out(2, 1)
    down(0, 0)
    own_inner(3)
    need(2, 0)
    down(0, 1)
    finish(0, 0)
    need(2, 1)
    down(0, 2)
    finish(0, 1)
    pass_out(2, 2)
    own_outer(3)
    own_inner(4)
    own_inner(5, True)
    load_merged.wait()
    load_gain2.wait()
    land(0, 0)
    need(2, 2)
    down(0, 3)
    finish(0, 2)
    land(0, 1)
    pass_in(3)
    pass_out(3, 1)
    finish(0, 3)
    land(0, 2)
    land(0, 3)

    for h in range(2):
        @pl.loop(0, quarter // step)
        def _(i):
            at = pl.ds(pl.multiple_of(h * quarter + i * step, step), step)
            full = pl.ds(pl.multiple_of(t * half + h * quarter + i * step, step), step)
            scale = lax.rsqrt(jnp.sum(ssq[at, :], axis=-1, keepdims=True) / width + EPS)
            normed2[0, full, :] = (middle[at, :] * scale * gain2[...]).astype(BF16)

        ag(1, 2 - h, h).start()
        ag(1, 1 + h, h).start()
        relay(1, 0, h, t).start()

    pass_out(3, 2)
    own_outer(4)
    pass_in(4)
    pass_out(4, 1)
    ag_first(1)
    pass_out(4, 2)
    own_outer(5, True)
    pass_in(5)
    pass_out(5, 1)
    ag_second(1)

    @on_mid
    def _():
        came(5, 1).wait_recv()
        for k in range(2):
            last_half(k).start()

    ag_far(1)

    make_hidden(1)
    for c in range(LINE):
        for r in range(PLANE):
            to_sibling(0, c, r).wait_send()
        for kind in range(6):
            rs(0, c, kind).wait_send()
    down(1, 0)
    need(5, 0)
    down(1, 1)
    finish(1, 0)
    need(5, 1)
    down(1, 2)
    finish(1, 1)
    land(1, 0)
    need_half(0)
    down(1, 3)
    finish(1, 2)
    land(1, 1)
    need_half(1)
    down(1, 4)
    finish(1, 3)
    land(1, 2)
    finish(1, 4)
    land(1, 3)
    land(1, 4)

    for m in range(6):
        for r in (1, 2, 3):
            p1(m, r).wait_send()
        to_inner(m).wait_send()

        @on_mid
        def _():
            to_outer(m).wait_send()
            on_inner(m).wait_send()
            on_outer(m, 1).wait_send()
            if m < 5:
                on_outer(m, 2).wait_send()
            else:
                last_half(0).wait_send()
                last_half(1).wait_send()

    for f in range(2):
        for h in range(2):
            for r in (1, 2):
                ag(f, r, h).wait_send()
            ag_on(f, h).wait_send()
            for r in range(1 - f, PLANE):
                relay(f, r, h, t).wait_send()
    for c in range(LINE + 1):
        for r in range(PLANE):
            to_sibling(1, c, r).wait_send()
        for kind in range(6):
            rs(1, c, kind).wait_send()
    for c in range(LINE + 1):
        out_across(c).wait_recv()
        at = lanes[1][c]
        out[other, at] = fin[:, at]
    for c in range(LINE + 1):
        out_across(c).wait_send()


def plane_shards(tokens, merged, gain1, g1, u1, d1, gain2, g2, u2, d2):
    rows, width = tokens.shape
    half = rows // 2
    hid, ds = d1.shape
    q = hid // PLANE
    far = pl.BlockSpec(memory_space=pl.ANY)
    dma = lambda *s: pltpu.SemaphoreType.DMA(s)
    return pl.pallas_call(
        kernel,
        out_shape=pltpu.VMEM((rows, width), BF16),
        in_specs=[far] * 10,
        out_specs=pl.BlockSpec(memory_space=pltpu.VMEM),
        scratch_shapes=[
            pltpu.VMEM((4, ds, hid), BF16),
            pltpu.VMEM((4, hid, ds), BF16),
            pltpu.VMEM((2, hid, ds), BF16),
            pltpu.VMEM((rows, width), BF16),
            pltpu.VMEM((rows, width), BF16),
            pltpu.VMEM((1, width), F32),
            pltpu.VMEM((1, width), F32),
            pltpu.VMEM((half, width), BF16),
            pltpu.VMEM((6, q, width), BF16),
            pltpu.VMEM((PLANE, rows, width), BF16),
            pltpu.VMEM((PLANE, rows, width), BF16),
            pltpu.VMEM((PLANE, rows, q), F32),
            pltpu.VMEM((PLANE, rows, q), F32),
            pltpu.VMEM((PLANE, rows, q), BF16),
            pltpu.VMEM((PLANE, half, width), BF16),
            pltpu.VMEM((PLANE, half, width), BF16),
            pltpu.VMEM((PLANE, half, width), BF16),
            pltpu.VMEM((PLANE - 1, half, width), BF16),
            pltpu.VMEM((2, half // 2, width), BF16),
            pltpu.VMEM((2, half, width), BF16),
            pltpu.VMEM((half, width), F32),
            pltpu.VMEM((half, 128), F32),
            dma(10), dma(6, 3), dma(6, 3), dma(6, 6), dma(6, 5),
            dma(2, 3, 2), dma(2, 3, 2), dma(2, 4, 2), dma(2, 4, 2),
            dma(2, LINE + 1, 4), dma(2, LINE + 1, 4), dma(2, LINE + 1, 6), dma(2, LINE + 1, 6),
            dma(LINE + 1), dma(LINE + 1),
        ],
        compiler_params=pltpu.CompilerParams(
            collective_id=0, has_side_effects=True, vmem_limit_bytes=60 * 2**20
        ),
    )(tokens, merged, gain1[None], gain2[None], g1, u1, d1, g2, u2, d2)


def shards(n_fs, n_tp, *args):
    rows, width = args[0].shape
    hid, cols = args[5].shape
    fits = n_fs == PLANE * LINE and n_tp == 2 and cols % 128 == 0
    fits = fits and hid % (32 * PLANE) == 0 and rows % 64 == 0
    return plane_shards(*args) if fits else gathered_shards(*args)


def solution(mesh):
    return jax.shard_map(
        functools.partial(shards, mesh.shape["fs"], mesh.shape["tp"]),
        mesh=mesh,
        in_specs=(
            P("fs", None),
            P("fs", None),
            P(),
            P("fs", "tp"),
            P("fs", "tp"),
            P("tp", "fs"),
            P(),
            P("fs", "tp"),
            P("fs", "tp"),
            P("tp", "fs"),
        ),
        out_specs=P("fs", None),
        check_vma=False,
    )
```

```python
import functools

import jax
import jax.numpy as jnp
from jax import lax
from jax.experimental import pallas as pl
from jax.experimental.pallas import tpu as pltpu
from jax.sharding import PartitionSpec as P

EPS = 1e-06
BF16 = jnp.bfloat16
F32 = jnp.float32
PLANE = 4
LINE = 4
PARTS = 2


def norm_rows(values, gain):
    scale = lax.rsqrt(jnp.mean(values * values, axis=-1, keepdims=True) + EPS)
    return values * scale * gain


def gathered_block(normed, gate, up, down):
    gate_whole = lax.all_gather(gate, "fs", axis=0, tiled=True)
    up_whole = lax.all_gather(up, "fs", axis=0, tiled=True)
    g = jnp.dot(normed, gate_whole, preferred_element_type=F32)
    u = jnp.dot(normed, up_whole, preferred_element_type=F32)
    hidden = (jax.nn.silu(g) * u).astype(BF16)
    down_whole = lax.all_gather(down, "fs", axis=1, tiled=True)
    part = jnp.dot(hidden, down_whole, preferred_element_type=F32)
    return lax.psum(part.astype(BF16), "tp").astype(F32)


def gathered_shards(tokens, merged, gain1, g1, u1, d1, gain2, g2, u2, d2):
    source = tokens.astype(F32)
    middle = source + merged.astype(F32)
    normed = norm_rows(source, gain1).astype(BF16)
    middle = middle + 0.5 * gathered_block(normed, g1, u1, d1)
    normed = norm_rows(middle, gain2).astype(BF16)
    return (middle + 0.5 * gathered_block(normed, g2, u2, d2)).astype(BF16)


def kernel(
    tokens_h, merged_h, gain1_h, gain2_h, wa, wb, wc, wd, we, wf, out_h,
    raw, turned, straight, tokens, merged, gain1, gain2, here, fin, w, normed1, normed2, acc_g, acc_u, hidden,
    prod, sib, comb, diag, rsr, middle, ssq,
    load, p1_s, p1_r, z_s, z_r,
    ag_s, ag_r, rel_s, rel_r, sib_s, sib_r, rs_s, rs_r, fin_s, fin_r, store,
):
    weights_in = (wa, wb, wc, wd, we, wf)
    fs = lax.axis_index("fs")
    t = lax.axis_index("tp")
    z = fs // PLANE
    p = fs % PLANE
    rows, width = tokens.shape
    half = rows // 2
    quarter = half // 2
    q, pw = w.shape[1], width // LINE
    ds = wc.shape[1]
    step = 16

    def dev(zz, pp, tt):
        return {"fs": zz * PLANE + pp, "tp": tt}

    peers = (p, p + 1 - 2 * (p % 2), (p + 2) % PLANE, PLANE - 1 - p)
    to_peer = [dev(z, pp, t) for pp in peers]
    sibling = dev(z, p, 1 - t)

    low = (z < 2).astype(jnp.int32)
    toward = 2 * low - 1
    mid = (z % 3 != 0).astype(jnp.int32)
    zi, zo = z + toward, z - toward * mid
    inner, outer = dev(zi, p, t), dev(zo, p, t)

    def on_mid(f):
        pl.when(mid == 1)(f)

    def on_end(f):
        pl.when(mid == 0)(f)

    def remote(src, dst, s, r, to):
        return pltpu.make_async_remote_copy(
            src_ref=src, dst_ref=dst, send_sem=s, recv_sem=r,
            device_id=to, device_id_type=pl.DeviceIdType.MESH,
        )

    mine = pl.ds(pl.multiple_of(t * half, 16), half)
    other = pl.ds(pl.multiple_of((1 - t) * half, 16), half)

    def shard_of(m):
        k = m // 3
        return straight.at[k] if m % 3 == 2 else turned.at[2 * k + m % 3]

    def loading(m):
        k = m // 3
        return pltpu.make_async_copy(
            weights_in[m], straight.at[k] if m % 3 == 2 else raw.at[2 * k + m % 3], load.at[m]
        )

    load_tokens = pltpu.make_async_copy(tokens_h, tokens, load.at[6])
    load_merged = pltpu.make_async_copy(merged_h, merged, load.at[7])
    load_gain1 = pltpu.make_async_copy(gain1_h, gain1, load.at[8])
    load_gain2 = pltpu.make_async_copy(gain2_h, gain2, load.at[9])
    for m in (0, 1):
        loading(m).start()
    load_tokens.start()
    load_gain1.start()
    for m in (2, 3, 4, 5):
        loading(m).start()
    load_merged.start()
    load_gain2.start()

    barrier = pltpu.get_barrier_semaphore()
    targets = [inner, sibling] + to_peer[1:]
    for to in targets:
        pl.semaphore_signal(barrier, inc=1, device_id=to, device_id_type=pl.DeviceIdType.MESH)

    @on_mid
    def _():
        pl.semaphore_signal(barrier, inc=1, device_id=outer, device_id_type=pl.DeviceIdType.MESH)

    def turn(m):
        k = 2 * (m // 3) + m % 3
        loading(m).wait()
        for j in range(raw.shape[2] // 128):
            turned[k, j * 128:(j + 1) * 128, :] = raw[k, :, j * 128:(j + 1) * 128].T

    def lanes_of(zz, pp):
        return pl.ds(pl.multiple_of((zz * PLANE + pp) * ds, ds), ds)

    def p1_sem(m, r):
        return p1_r.at[3 * m + r - 1 if m < 2 else 4 + m]

    def p1(m, r):
        src = shard_of(m).at[pl.ds(pl.multiple_of(peers[r] * q, 16), q), :]
        return remote(src, w.at[m, :, lanes_of(z, p)], p1_s.at[0], p1_sem(m, r), to_peer[r])

    def p1_in(m, r):
        src = w.at[m, :, lanes_of(z, peers[r])]
        return remote(src, src, p1_s.at[0], p1_sem(m, r), to_peer[r])

    def p1_whole(m):
        src = w.at[m, :, pl.ds(0, (PLANE - 1) * ds)]
        return remote(src, src, p1_s.at[0], p1_sem(m, 1), to_peer[1])

    def place(m):
        w[m, :, lanes_of(z, p)] = shard_of(m)[pl.ds(pl.multiple_of(p * q, 16), q), :]

    def start_p1(m):
        for r in (3, 1, 2):
            p1(m, r).start()

    def blk(m, zz):
        return w.at[m, :, pl.ds(pl.multiple_of(zz * pw, pw), pw)]

    first_slot = 3 * (1 - mid)
    wide = 1 + 3 * PARTS

    def z_sem(m, slot):
        return z_r.at[4 * m + (m // 3) * (wide - 4) + slot]

    def to_inner(m, r=None):
        at = blk(m, z) if r is None else w.at[m, :, lanes_of(z, peers[r])]
        return remote(at, at, z_s.at[0], z_sem(m, first_slot), inner)

    def to_outer(m, r):
        at = w.at[m, :, lanes_of(z, peers[r])]
        return remote(at, at, z_s.at[1], z_sem(m, 0), outer)

    def on_inner(m):
        return remote(blk(m, zo), blk(m, zo), z_s.at[0], z_sem(m, 1), inner)

    def cuts(m):
        return PARTS if m % 3 == 2 else 1

    def part_blk(m, zz, k):
        n = pw // cuts(m)
        return w.at[m, :, pl.ds(pl.multiple_of(zz * pw + k * n, n), n)]

    def outward(m, d, k):
        at = part_blk(m, z + d * toward, k)
        return remote(at, at, z_s.at[1], z_sem(m, d if k == 0 else 1 + d + 3 * k), outer)

    def came(m, slot):
        zz = zo if slot == 3 else z + (slot + 1) * toward
        return remote(blk(m, zz), blk(m, zz), z_s.at[0], z_sem(m, slot), inner)

    def came_part(m, slot, k):
        at = part_blk(m, z + (slot + 1) * toward, k)
        return remote(at, at, z_s.at[0], z_sem(m, slot if k == 0 else 1 + slot + 3 * k), inner)

    def piece_out(m, r):
        to_inner(m, r).start()

        @on_mid
        def _():
            to_outer(m, r).start()

    def own_now(m):
        for r in (1, 2, 3):
            p1_in(m, r).wait_recv()
            piece_out(m, r)

    def own_inner(m):
        p1_whole(m).wait_recv()
        to_inner(m).start()

    def own_outer(m):
        @on_mid
        def _():
            for k in range(cuts(m)):
                outward(m, 0, k).start()

    def pass_in(m):
        @on_mid
        def _():
            came(m, 3).wait_recv()
            on_inner(m).start()

    def pass_out(m, d):
        @on_mid
        def _():
            came(m, d - 1).wait_recv()
            for k in range(cuts(m)):
                outward(m, d, k).start()

    def need(f, c):
        if c >= PARTS:
            @on_end
            def _():
                came_part(3 * f + 2, c // PARTS - 1, c % PARTS).wait_recv()

    def drain(sem, ref):
        remote(ref, ref, sem, sem, sibling).wait_send()

    bufs = (normed1, normed2)

    def piece(tt, h):
        return pl.ds(pl.multiple_of(tt * half + h * quarter, 16), quarter)

    def ag(f, r, h):
        at = piece(t, h)
        return remote(bufs[f].at[0, at, :], bufs[f].at[r, at, :], ag_s.at[0], ag_r.at[r - 1, h], to_peer[r])

    def ag_on(f, h):
        at = piece(t, h)
        return remote(bufs[f].at[2 - h, at, :], bufs[f].at[3, at, :], ag_s.at[0], ag_r.at[2, h], to_peer[1 + h])

    def relay(f, r, h, tt):
        at = bufs[f].at[r, piece(tt, h), :]
        return remote(at, at, rel_s.at[0], rel_r.at[r], sibling)

    def ag_first(f):
        for r, h in ((2, 0), (1, 1)):
            ag(f, r, h).wait_recv()
            ag_on(f, h).start()
            relay(f, r, h, t).start()

    def ag_second(f):
        for r, h in ((2, 1), (1, 0)):
            ag(f, r, h).wait_recv()
            relay(f, r, h, t).start()

    def ag_far(f):
        for h in range(2):
            ag_on(f, h).wait_recv()
            relay(f, 3, h, t).start()

    zs = (z, zi, jnp.where(mid == 1, zo, z + 2 * toward), jnp.where(mid == 1, z + 2 * toward, z + 3 * toward))
    cwid = pw // PARTS
    chunks = LINE * PARTS
    lanes = [pl.ds(pl.multiple_of(zz * pw + k * cwid, cwid), cwid) for zz in zs for k in range(PARTS)]
    lanes_a = pl.ds(pl.multiple_of((1 - low) * pw, pw), 3 * pw)
    lanes_b = pl.ds(pl.multiple_of(low * 3 * pw, pw), pw)
    first, second = pl.ds(0, quarter), pl.ds(quarter, quarter)

    def to_sibling(f, c, r):
        return remote(prod.at[r, other, lanes[c]], sib.at[r, :, lanes[c]], sib_s.at[0], sib_r.at[c % 2, r], sibling)

    def rs(f, c, kind):
        at = lanes[c]
        src, dst, r = (
            (comb.at[2, first, at], diag.at[0, :, at], 1),
            (comb.at[2, second, at], diag.at[1, :, at], 2),
            (comb.at[0, first, at], rsr.at[0, first, at], 1),
            (comb.at[0, second, at], rsr.at[0, second, at], 1),
            (comb.at[1, second, at], rsr.at[1, second, at], 2),
            (comb.at[1, first, at], rsr.at[1, first, at], 2),
        )[kind]
        return remote(src, dst, rs_s.at[0], rs_r.at[c, min(kind, 2)], to_peer[r])

    def product(f, k, r, at):
        dims = (((1,), (1,)), ((), ()))
        return lax.dot_general(bufs[f][r, :, at], w[3 * f + k, :, at], dims, preferred_element_type=F32)

    def slot_in(f, r):
        @pl.when(r > (0 if f == 0 else -1))
        def _():
            at = bufs[f].at[r, other, :]
            remote(at, at, rel_s.at[0], rel_r.at[r], sibling).wait_recv()

    def silu(g):
        return g / (1.0 + jnp.exp(-g))

    every = slice(None)

    def begin_hidden(f, lo, hi):
        @pl.loop(lo, hi)
        def _(r):
            slot_in(f, r)
            acc_g[r] = silu(product(f, 0, r, every))
            acc_u[r] = product(f, 1, r, lanes_a)

    def end_hidden(f):
        @pl.loop(0, PLANE)
        def _(r):
            u = acc_u[r] + product(f, 1, r, lanes_b)
            hidden[r] = (acc_g[r] * u).astype(BF16)

    def whole_hidden(f, lo, hi):
        @pl.loop(lo, hi)
        def _(r):
            slot_in(f, r)
            g = silu(product(f, 0, r, every))
            hidden[r] = (g * product(f, 1, r, every)).astype(BF16)

    def all_came(*pairs):
        @on_end
        def _():
            for m, slot in pairs:
                came(m, slot).wait_recv()

    def down(f, c):
        at = lanes[c]

        @pl.loop(0, PLANE)
        def _(k):
            r = PLANE - 1 - k
            prod[r, :, at] = jnp.dot(hidden[r], w[3 * f + 2, :, at], preferred_element_type=F32).astype(BF16)
            to_sibling(f, c, r).start()

        for r, kinds in ((3, (0, 1)), (2, (4,)), (1, (2,))):
            to_sibling(f, c, r).wait_recv()

            @pl.loop(0, half // (2 * step))
            def _(i):
                some = pl.ds(pl.multiple_of(i * 2 * step, step), 2 * step)
                full = pl.ds(pl.multiple_of(t * half + i * 2 * step, step), 2 * step)
                comb[r - 1, some, at] = (prod[r, full, at].astype(F32) + sib[r, some, at].astype(F32)).astype(BF16)

            for kind in kinds:
                rs(f, c, kind).start()
        to_sibling(f, c, 0).wait_recv()

    def finish(f, c):
        at = lanes[c]
        rs(f, c, 0).wait_recv()
        comb[1, first, at] = (comb[1, first, at].astype(F32) + diag[0, :, at].astype(F32)).astype(BF16)
        rs(f, c, 5).start()
        rs(f, c, 1).wait_recv()
        comb[0, second, at] = (comb[0, second, at].astype(F32) + diag[1, :, at].astype(F32)).astype(BF16)
        rs(f, c, 3).start()

    def reduced(rows_at, full, at):
        total = prod[0, full, at].astype(F32) + sib[0, rows_at, at].astype(F32)
        return total + rsr[0, rows_at, at].astype(F32) + rsr[1, rows_at, at].astype(F32)

    def out_across(c):
        at = lanes[c]
        return remote(here.at[:, at], fin.at[:, at], fin_s.at[0], fin_r.at[c], sibling)

    def out_store(c, k):
        at = lanes[c]
        return pltpu.make_async_copy((here, fin)[k].at[:, at], out_h.at[(mine, other)[k], at], store.at[0])

    def store_other(c):
        out_across(c).wait_recv()
        out_store(c, 1).start()

    def land(f, c):
        at = lanes[c]
        remote(rsr.at[:, :, at], rsr.at[:, :, at], rs_s.at[0], rs_r.at[c, 2], sibling).wait_recv()

        @pl.loop(0, half // (2 * step))
        def _(i):
            some = pl.ds(pl.multiple_of(i * 2 * step, step), 2 * step)
            full = pl.ds(pl.multiple_of(t * half + i * 2 * step, step), 2 * step)
            if f == 0:
                value = tokens[full, at].astype(F32) + merged[full, at].astype(F32) + 0.5 * reduced(some, full, at)
                middle[some, at] = value
                squares = value * value
                sums = sum(squares[:, k * 128:(k + 1) * 128] for k in range(cwid // 128))
                ssq[some, :] = sums if c == 0 else ssq[some, :] + sums
            else:
                here[some, at] = (middle[some, at] + 0.5 * reduced(some, full, at)).astype(BF16)

        if f == 1:
            out_across(c).start()
            out_store(c, 0).start()

    def norm_first(start, count):
        @pl.loop(0, count // step)
        def _(i):
            at = pl.ds(pl.multiple_of(start + i * step, step), step)
            normed1[0, at, :] = norm_rows(tokens[at, :].astype(F32), gain1[...]).astype(BF16)

    turn(0)
    place(0)
    pl.semaphore_wait(barrier, len(targets) + mid)
    start_p1(0)
    piece_out(0, 0)
    turn(1)
    start_p1(1)
    place(1)
    piece_out(1, 0)

    load_tokens.wait()
    load_gain1.wait()
    norm_first(t * half, half)
    for r, h in ((2, 0), (1, 1), (2, 1), (1, 0)):
        ag(0, r, h).start()
    loading(2).wait()
    start_p1(2)
    place(2)
    own_now(0)
    norm_first((1 - t) * half, half)
    own_now(1)
    turn(3)
    turn(4)
    pass_in(0)
    pass_out(0, 1)
    pass_in(1)
    pass_out(1, 1)
    ag_first(0)
    loading(5).wait()
    for m in (3, 4, 5):
        start_p1(m)
        place(m)
    pass_out(0, 2)
    ag_second(0)
    own_inner(2)
    begin_hidden(0, 0, 3 * mid)
    pass_out(1, 2)
    own_outer(2)
    ag_far(0)

    all_came((0, 0), (0, 1), (0, 2), (1, 0), (1, 1))
    begin_hidden(0, 3 * mid, PLANE)

    @on_end
    def _():
        for m in (3, 4, 5):
            own_inner(m)

    all_came((1, 2))
    end_hidden(0)
    pass_in(2)
    pass_out(2, 1)

    @on_mid
    def _():
        own_inner(3)

    down(0, 0)
    down(0, 1)
    finish(0, 0)
    for c in range(2, chunks):
        need(0, c)
        down(0, c)
        finish(0, c - 1)
        if c == 3:
            load_merged.wait()
            load_gain2.wait()
        if c >= 3:
            land(0, c - 3)
        if c == 4:
            pass_out(2, 2)
            own_outer(3)
        if c == 5:
            pass_in(3)
            pass_out(3, 1)

            @on_mid
            def _():
                own_inner(4)

    land(0, 5)
    finish(0, 7)
    pass_in(4)

    @on_mid
    def _():
        own_inner(5)

    land(0, 6)
    land(0, 7)
    drain(ag_s.at[0], normed1.at[pl.ds(0, 3), pl.ds(0, half), :])
    drain(rel_s.at[0], normed1.at[pl.ds(0, 3), pl.ds(0, half), :])

    @pl.loop(0, half // step)
    def _(i):
        at = pl.ds(pl.multiple_of(i * step, step), step)
        full = pl.ds(pl.multiple_of(t * half + i * step, step), step)
        scale = lax.rsqrt(jnp.sum(ssq[at, :], axis=-1, keepdims=True) / width + EPS)
        normed2[0, full, :] = (middle[at, :] * scale * gain2[...]).astype(BF16)

    for r, h in ((2, 0), (1, 1), (2, 1), (1, 0)):
        ag(1, r, h).start()
    for h in range(2):
        relay(1, 0, h, t).start()
    pass_out(3, 2)
    own_outer(4)
    pass_in(5)
    pass_out(4, 1)
    ag_first(1)
    pass_out(4, 2)
    own_outer(5)
    ag_second(1)
    pass_out(5, 1)

    @on_mid
    def _():
        whole_hidden(1, 0, 3)

    all_came((3, 0), (3, 1), (3, 2), (4, 0), (4, 1))
    begin_hidden(1, 0, 3 - 3 * mid)
    ag_far(1)
    drain(sib_s.at[0], sib)
    drain(rs_s.at[0], comb)

    @on_mid
    def _():
        whole_hidden(1, 3, 4)

    pass_out(5, 2)

    @on_end
    def _():
        begin_hidden(1, 3, 4)
        came(4, 2).wait_recv()
        end_hidden(1)

    down(1, 0)
    down(1, 1)
    finish(1, 0)
    for c in range(2, chunks):
        need(1, c)
        down(1, c)
        finish(1, c - 1)
        if 3 <= c < chunks - 1:
            land(1, c - 3)
    land(1, chunks - 4)
    land(1, chunks - 3)
    for c in range(chunks - 4):
        store_other(c)
    finish(1, chunks - 1)
    land(1, chunks - 2)
    land(1, chunks - 1)

    for c in range(chunks - 4, chunks):
        store_other(c)
    drain(p1_s.at[0], w.at[:, :, pl.ds(0, (PLANE - 1) * ds)])

    @on_mid
    def _():
        drain(z_s.at[0], w.at[:, :, pl.ds(0, 2 * pw)])
        drain(z_s.at[1], w.at[:, :, pl.ds(0, 3 * pw)])

    @on_end
    def _():
        drain(z_s.at[0], w.at[:, :, pl.ds(0, pw)])

    drain(ag_s.at[0], normed2.at[pl.ds(0, 3), pl.ds(0, half), :])
    drain(rel_s.at[0], normed2.at[:, pl.ds(0, half), :])
    drain(sib_s.at[0], sib)
    drain(rs_s.at[0], comb)
    drain(fin_s.at[0], here)
    pltpu.make_async_copy(tokens, tokens, store.at[0]).wait()


def plane_shards(tokens, merged, gain1, g1, u1, d1, gain2, g2, u2, d2):
    rows, width = tokens.shape
    half = rows // 2
    hid, ds = d1.shape
    q = hid // PLANE
    chunks = LINE * PARTS
    far = pl.BlockSpec(memory_space=pl.ANY)
    dma = lambda *s: pltpu.SemaphoreType.DMA(s)
    return pl.pallas_call(
        kernel,
        out_shape=pltpu.VMEM((rows, width), BF16),
        in_specs=[far] * 10,
        out_specs=far,
        scratch_shapes=[
            pltpu.VMEM((4, ds, hid), BF16),
            pltpu.VMEM((4, hid, ds), BF16),
            pltpu.VMEM((2, hid, ds), BF16),
            pltpu.VMEM((rows, width), BF16),
            pltpu.VMEM((rows, width), BF16),
            pltpu.VMEM((1, width), F32),
            pltpu.VMEM((1, width), F32),
            pltpu.VMEM((half, width), BF16),
            pltpu.VMEM((half, width), BF16),
            pltpu.VMEM((6, q, width), BF16),
            pltpu.VMEM((PLANE, rows, width), BF16),
            pltpu.VMEM((PLANE, rows, width), BF16),
            pltpu.VMEM((PLANE, rows, q), F32),
            pltpu.VMEM((PLANE, rows, q), F32),
            pltpu.VMEM((PLANE, rows, q), BF16),
            pltpu.VMEM((PLANE, rows, width), BF16),
            pltpu.VMEM((PLANE, half, width), BF16),
            pltpu.VMEM((PLANE - 1, half, width), BF16),
            pltpu.VMEM((2, half // 2, width), BF16),
            pltpu.VMEM((2, half, width), BF16),
            pltpu.VMEM((half, width), F32),
            pltpu.VMEM((half, 128), F32),
            dma(10), dma(1), dma(10), dma(2), dma(24 + 2 * (3 * PARTS - 3)),
            dma(1), dma(3, 2), dma(1), dma(PLANE),
            dma(1), dma(2, PLANE), dma(1), dma(chunks, 3),
            dma(1), dma(chunks), dma(1),
        ],
        compiler_params=pltpu.CompilerParams(
            collective_id=0, has_side_effects=True, vmem_limit_bytes=60 * 2**20
        ),
    )(tokens, merged, gain1[None], gain2[None], g1, u1, d1, g2, u2, d2)


def shards(n_fs, n_tp, *args):
    rows, width = args[0].shape
    hid, cols = args[5].shape
    fits = n_fs == PLANE * LINE and n_tp == 2 and cols % 128 == 0 and width % (128 * LINE * PARTS) == 0
    fits = fits and hid % (32 * PLANE) == 0 and rows % 64 == 0
    return plane_shards(*args) if fits else gathered_shards(*args)


def solution(mesh):
    return jax.shard_map(
        functools.partial(shards, mesh.shape["fs"], mesh.shape["tp"]),
        mesh=mesh,
        in_specs=(
            P("fs", None),
            P("fs", None),
            P(),
            P("fs", "tp"),
            P("fs", "tp"),
            P("tp", "fs"),
            P(),
            P("fs", "tp"),
            P("fs", "tp"),
            P("tp", "fs"),
        ),
        out_specs=P("fs", None),
        check_vma=False,
    )
```

```python
import functools

import jax
import jax.numpy as jnp
from jax import lax
from jax.experimental import pallas as pl
from jax.experimental.pallas import tpu as pltpu
from jax.sharding import PartitionSpec as P

EPS = 1e-06
BF16 = jnp.bfloat16
F32 = jnp.float32
PLANE = 4
LINE = 4
PARTS = 2


def norm_rows(values, gain):
    scale = lax.rsqrt(jnp.mean(values * values, axis=-1, keepdims=True) + EPS)
    return values * scale * gain


def gathered_block(normed, gate, up, down):
    gate_whole = lax.all_gather(gate, "fs", axis=0, tiled=True)
    up_whole = lax.all_gather(up, "fs", axis=0, tiled=True)
    g = jnp.dot(normed, gate_whole, preferred_element_type=F32)
    u = jnp.dot(normed, up_whole, preferred_element_type=F32)
    hidden = (jax.nn.silu(g) * u).astype(BF16)
    down_whole = lax.all_gather(down, "fs", axis=1, tiled=True)
    part = jnp.dot(hidden, down_whole, preferred_element_type=F32)
    return lax.psum(part.astype(BF16), "tp").astype(F32)


def gathered_shards(tokens, merged, gain1, g1, u1, d1, gain2, g2, u2, d2):
    source = tokens.astype(F32)
    middle = source + merged.astype(F32)
    normed = norm_rows(source, gain1).astype(BF16)
    middle = middle + 0.5 * gathered_block(normed, g1, u1, d1)
    normed = norm_rows(middle, gain2).astype(BF16)
    return (middle + 0.5 * gathered_block(normed, g2, u2, d2)).astype(BF16)


def kernel(
    tokens_h, merged_h, gain1_h, gain2_h, wa, wb, wc, wd, we, wf, out_h,
    raw, turned, straight, tokens, merged, gain1, gain2, here, fin, w, normed1, normed2, acc_g, acc_u, hidden,
    prod, sib, comb, diag, rsr, middle, ssq,
    load, p1_s, p1_r, z_s, z_r,
    ag_s, ag_r, rel_s, rel_r, sib_s, sib_r, rs_s, rs_r, fin_s, fin_r, store,
):
    weights_in = (wa, wb, wc, wd, we, wf)
    fs = lax.axis_index("fs")
    t = lax.axis_index("tp")
    z = fs // PLANE
    p = fs % PLANE
    rows, width = tokens.shape
    half = rows // 2
    quarter = half // 2
    q, pw = w.shape[1], width // LINE
    ds = wc.shape[1]
    step = 16

    def dev(zz, pp, tt):
        return {"fs": zz * PLANE + pp, "tp": tt}

    peers = (p, p + 1 - 2 * (p % 2), (p + 2) % PLANE, PLANE - 1 - p)
    to_peer = [dev(z, pp, t) for pp in peers]
    sibling = dev(z, p, 1 - t)

    low = (z < 2).astype(jnp.int32)
    toward = 2 * low - 1
    mid = (z % 3 != 0).astype(jnp.int32)
    zi, zo = z + toward, z - toward * mid
    inner, outer = dev(zi, p, t), dev(zo, p, t)

    def on_mid(f):
        pl.when(mid == 1)(f)

    def on_end(f):
        pl.when(mid == 0)(f)

    def remote(src, dst, s, r, to):
        return pltpu.make_async_remote_copy(
            src_ref=src, dst_ref=dst, send_sem=s, recv_sem=r,
            device_id=to, device_id_type=pl.DeviceIdType.MESH,
        )

    mine = pl.ds(pl.multiple_of(t * half, 16), half)
    other = pl.ds(pl.multiple_of((1 - t) * half, 16), half)

    def shard_of(m):
        k = m // 3
        return straight.at[k] if m % 3 == 2 else turned.at[2 * k + m % 3]

    def loading(m):
        k = m // 3
        return pltpu.make_async_copy(
            weights_in[m], straight.at[k] if m % 3 == 2 else raw.at[2 * k + m % 3], load.at[m]
        )

    load_tokens = pltpu.make_async_copy(tokens_h, tokens, load.at[6])
    load_merged = pltpu.make_async_copy(merged_h, merged, load.at[7])
    load_gain1 = pltpu.make_async_copy(gain1_h, gain1, load.at[8])
    load_gain2 = pltpu.make_async_copy(gain2_h, gain2, load.at[9])
    for m in (0, 1):
        loading(m).start()
    load_tokens.start()
    load_gain1.start()
    for m in (3, 4, 2, 5):
        loading(m).start()
    load_merged.start()
    load_gain2.start()

    barrier = pltpu.get_barrier_semaphore()
    targets = [inner, sibling] + to_peer[1:]
    for to in targets:
        pl.semaphore_signal(barrier, inc=1, device_id=to, device_id_type=pl.DeviceIdType.MESH)

    @on_mid
    def _():
        pl.semaphore_signal(barrier, inc=1, device_id=outer, device_id_type=pl.DeviceIdType.MESH)

    def turn(m):
        k = 2 * (m // 3) + m % 3
        loading(m).wait()
        for j in range(raw.shape[2] // 128):
            turned[k, j * 128:(j + 1) * 128, :] = raw[k, :, j * 128:(j + 1) * 128].T

    def lanes_of(zz, pp):
        return pl.ds(pl.multiple_of((zz * PLANE + pp) * ds, ds), ds)

    def p1_sem(m, r):
        return p1_r.at[3 * m + r - 1 if m < 2 else 4 + m]

    def p1(m, r):
        src = shard_of(m).at[pl.ds(pl.multiple_of(peers[r] * q, 16), q), :]
        return remote(src, w.at[m, :, lanes_of(z, p)], p1_s.at[0], p1_sem(m, r), to_peer[r])

    def p1_in(m, r):
        src = w.at[m, :, lanes_of(z, peers[r])]
        return remote(src, src, p1_s.at[0], p1_sem(m, r), to_peer[r])

    def p1_whole(m):
        src = w.at[m, :, pl.ds(0, (PLANE - 1) * ds)]
        return remote(src, src, p1_s.at[0], p1_sem(m, 1), to_peer[1])

    def place(m):
        w[m, :, lanes_of(z, p)] = shard_of(m)[pl.ds(pl.multiple_of(p * q, 16), q), :]

    def start_p1(m):
        for r in (3, 1, 2):
            p1(m, r).start()

    def blk(m, zz):
        return w.at[m, :, pl.ds(pl.multiple_of(zz * pw, pw), pw)]

    first_slot = 3 * (1 - mid)
    wide = 1 + 3 * PARTS

    def z_sem(m, slot):
        return z_r.at[4 * m + (m // 3) * (wide - 4) + slot]

    def to_inner(m, r=None):
        at = blk(m, z) if r is None else w.at[m, :, lanes_of(z, peers[r])]
        return remote(at, at, z_s.at[0], z_sem(m, first_slot), inner)

    def to_outer(m, r):
        at = w.at[m, :, lanes_of(z, peers[r])]
        return remote(at, at, z_s.at[1], z_sem(m, 0), outer)

    def on_inner(m):
        return remote(blk(m, zo), blk(m, zo), z_s.at[0], z_sem(m, 1), inner)

    def cuts(m):
        return PARTS if m % 3 == 2 else 1

    def part_blk(m, zz, k):
        n = pw // cuts(m)
        return w.at[m, :, pl.ds(pl.multiple_of(zz * pw + k * n, n), n)]

    def outward(m, d, k):
        at = part_blk(m, z + d * toward, k)
        return remote(at, at, z_s.at[1], z_sem(m, d if k == 0 else 1 + d + 3 * k), outer)

    early = (0, 1, 3, 4)

    def came(m, slot):
        zz = zo if slot == 3 else z + (slot + 1) * toward
        return remote(blk(m, zz), blk(m, zz), z_s.at[0], z_sem(m, slot), inner)

    def came_part(m, slot, k):
        at = part_blk(m, z + (slot + 1) * toward, k)
        return remote(at, at, z_s.at[0], z_sem(m, slot if k == 0 else 1 + slot + 3 * k), inner)

    def piece_out(m, r):
        to_inner(m, r).start()

        @on_mid
        def _():
            to_outer(m, r).start()

    def own_now(m):
        for r in (1, 2, 3):
            p1_in(m, r).wait_recv()
            piece_out(m, r)

    def own_inner(m):
        p1_whole(m).wait_recv()
        if m in early:
            for r in (1, 2, 3):
                to_inner(m, r).start()
        else:
            to_inner(m).start()

    def own_outer(m):
        @on_mid
        def _():
            if m in early:
                for r in (1, 2, 3):
                    to_outer(m, r).start()
            else:
                for k in range(cuts(m)):
                    outward(m, 0, k).start()

    def pass_in(m):
        @on_mid
        def _():
            came(m, 3).wait_recv()
            on_inner(m).start()

    def pass_out(m, d):
        @on_mid
        def _():
            came(m, d - 1).wait_recv()
            for k in range(cuts(m)):
                outward(m, d, k).start()

    def need(f, c):
        if c >= PARTS:
            @on_end
            def _():
                came_part(3 * f + 2, c // PARTS - 1, c % PARTS).wait_recv()

    def drain(sem, ref):
        remote(ref, ref, sem, sem, sibling).wait_send()

    bufs = (normed1, normed2)

    def piece(tt, h):
        return pl.ds(pl.multiple_of(tt * half + h * quarter, 16), quarter)

    def ag(f, r, h):
        at = piece(t, h)
        return remote(bufs[f].at[0, at, :], bufs[f].at[r, at, :], ag_s.at[0], ag_r.at[r - 1, h], to_peer[r])

    def ag_on(f, h):
        at = piece(t, h)
        return remote(bufs[f].at[2 - h, at, :], bufs[f].at[3, at, :], ag_s.at[0], ag_r.at[2, h], to_peer[1 + h])

    def relay(f, r, h, tt):
        at = bufs[f].at[r, piece(tt, h), :]
        return remote(at, at, rel_s.at[0], rel_r.at[r], sibling)

    def ag_first(f):
        for r, h in ((2, 0), (1, 1)):
            ag(f, r, h).wait_recv()
            ag_on(f, h).start()
            relay(f, r, h, t).start()

    def ag_second(f):
        for r, h in ((2, 1), (1, 0)):
            ag(f, r, h).wait_recv()
            relay(f, r, h, t).start()

    def ag_far(f):
        for h in range(2):
            ag_on(f, h).wait_recv()
            relay(f, 3, h, t).start()

    zs = (z, zi, jnp.where(mid == 1, zo, z + 2 * toward), jnp.where(mid == 1, z + 2 * toward, z + 3 * toward))
    cwid = pw // PARTS
    chunks = LINE * PARTS
    lanes = [pl.ds(pl.multiple_of(zz * pw + k * cwid, cwid), cwid) for zz in zs for k in range(PARTS)]
    lanes_a = pl.ds(pl.multiple_of((1 - low) * pw, pw), 3 * pw)
    lanes_b = pl.ds(pl.multiple_of(low * 3 * pw, pw), pw)
    first, second = pl.ds(0, quarter), pl.ds(quarter, quarter)

    def to_sibling(f, c, r):
        return remote(prod.at[r, other, lanes[c]], sib.at[r, :, lanes[c]], sib_s.at[0], sib_r.at[c % 2, r], sibling)

    def rs(f, c, kind):
        at = lanes[c]
        src, dst, r = (
            (comb.at[2, first, at], diag.at[0, :, at], 1),
            (comb.at[2, second, at], diag.at[1, :, at], 2),
            (comb.at[0, first, at], rsr.at[0, first, at], 1),
            (comb.at[0, second, at], rsr.at[0, second, at], 1),
            (comb.at[1, second, at], rsr.at[1, second, at], 2),
            (comb.at[1, first, at], rsr.at[1, first, at], 2),
        )[kind]
        return remote(src, dst, rs_s.at[0], rs_r.at[c, min(kind, 2)], to_peer[r])

    def product(f, k, r, at):
        dims = (((1,), (1,)), ((), ()))
        return lax.dot_general(bufs[f][r, :, at], w[3 * f + k, :, at], dims, preferred_element_type=F32)

    def slot_in(f, r):
        @pl.when(r > (0 if f == 0 else -1))
        def _():
            at = bufs[f].at[r, other, :]
            remote(at, at, rel_s.at[0], rel_r.at[r], sibling).wait_recv()

    def silu(g):
        return g / (1.0 + jnp.exp(-g))

    every = slice(None)

    def gate_slots(f, lo, hi):
        @pl.loop(lo, hi)
        def _(r):
            slot_in(f, r)
            acc_g[r] = silu(product(f, 0, r, every))

    def up_slots(f, lo, hi):
        @pl.loop(lo, hi)
        def _(r):
            acc_u[r] = product(f, 1, r, lanes_a)

    def begin_hidden(f, lo, hi):
        @pl.loop(lo, hi)
        def _(r):
            slot_in(f, r)
            acc_g[r] = silu(product(f, 0, r, every))
            acc_u[r] = product(f, 1, r, lanes_a)

    def first_product(f, r):
        prod[r, :, lanes[0]] = jnp.dot(hidden[r], w[3 * f + 2, :, lanes[0]], preferred_element_type=F32).astype(BF16)
        to_sibling(f, 0, r).start()

    def end_hidden(f):
        @pl.loop(0, PLANE)
        def _(k):
            r = PLANE - 1 - k
            u = acc_u[r] + product(f, 1, r, lanes_b)
            hidden[r] = (acc_g[r] * u).astype(BF16)
            first_product(f, r)

    def whole_hidden(f, lo, hi):
        @pl.loop(lo, hi)
        def _(r):
            slot_in(f, r)
            g = silu(product(f, 0, r, every))
            hidden[r] = (g * product(f, 1, r, every)).astype(BF16)
            first_product(f, r)

    def all_came(*pairs):
        @on_end
        def _():
            for m, slot in pairs:
                came(m, slot).wait_recv()

    def down(f, c):
        at = lanes[c]

        @pl.loop(0, PLANE if c else 0)
        def _(k):
            r = PLANE - 1 - k
            prod[r, :, at] = jnp.dot(hidden[r], w[3 * f + 2, :, at], preferred_element_type=F32).astype(BF16)
            to_sibling(f, c, r).start()

        for r, kinds in ((3, (0, 1)), (2, (4,)), (1, (2,))):
            to_sibling(f, c, r).wait_recv()

            @pl.loop(0, half // (2 * step))
            def _(i):
                some = pl.ds(pl.multiple_of(i * 2 * step, step), 2 * step)
                full = pl.ds(pl.multiple_of(t * half + i * 2 * step, step), 2 * step)
                comb[r - 1, some, at] = (prod[r, full, at].astype(F32) + sib[r, some, at].astype(F32)).astype(BF16)

            for kind in kinds:
                rs(f, c, kind).start()
        to_sibling(f, c, 0).wait_recv()

    def finish(f, c):
        at = lanes[c]
        rs(f, c, 0).wait_recv()
        comb[1, first, at] = (comb[1, first, at].astype(F32) + diag[0, :, at].astype(F32)).astype(BF16)
        rs(f, c, 5).start()
        rs(f, c, 1).wait_recv()
        comb[0, second, at] = (comb[0, second, at].astype(F32) + diag[1, :, at].astype(F32)).astype(BF16)
        rs(f, c, 3).start()

    def reduced(rows_at, full, at):
        total = prod[0, full, at].astype(F32) + sib[0, rows_at, at].astype(F32)
        return total + rsr[0, rows_at, at].astype(F32) + rsr[1, rows_at, at].astype(F32)

    def out_across(c):
        at = lanes[c]
        return remote(here.at[:, at], fin.at[:, at], fin_s.at[0], fin_r.at[c], sibling)

    def out_store(c, k):
        at = lanes[c]
        return pltpu.make_async_copy((here, fin)[k].at[:, at], out_h.at[(mine, other)[k], at], store.at[0])

    def store_other(c):
        out_across(c).wait_recv()
        out_store(c, 1).start()

    def land(f, c):
        at = lanes[c]
        remote(rsr.at[:, :, at], rsr.at[:, :, at], rs_s.at[0], rs_r.at[c, 2], sibling).wait_recv()

        @pl.loop(0, half // (2 * step))
        def _(i):
            some = pl.ds(pl.multiple_of(i * 2 * step, step), 2 * step)
            full = pl.ds(pl.multiple_of(t * half + i * 2 * step, step), 2 * step)
            if f == 0:
                value = tokens[full, at].astype(F32) + merged[full, at].astype(F32) + 0.5 * reduced(some, full, at)
                middle[some, at] = value
                squares = value * value
                sums = sum(squares[:, k * 128:(k + 1) * 128] for k in range(cwid // 128))
                ssq[some, :] = sums if c == 0 else ssq[some, :] + sums
            else:
                here[some, at] = (middle[some, at] + 0.5 * reduced(some, full, at)).astype(BF16)

        if f == 1:
            out_across(c).start()
            out_store(c, 0).start()

    def norm_first(start, count):
        @pl.loop(0, count // step)
        def _(i):
            at = pl.ds(pl.multiple_of(start + i * step, step), step)
            normed1[0, at, :] = norm_rows(tokens[at, :].astype(F32), gain1[...]).astype(BF16)

    turn(0)
    place(0)
    pl.semaphore_wait(barrier, len(targets) + mid)
    start_p1(0)
    piece_out(0, 0)
    turn(1)
    start_p1(1)
    place(1)
    piece_out(1, 0)
    for m in (3, 4):
        turn(m)
        place(m)
        piece_out(m, 0)

    load_tokens.wait()
    load_gain1.wait()
    norm_first(t * half, half)
    for r, h in ((2, 0), (1, 1), (2, 1), (1, 0)):
        ag(0, r, h).start()
    loading(2).wait()
    start_p1(2)
    place(2)
    own_now(0)
    norm_first((1 - t) * half, half)
    own_now(1)
    pass_in(0)
    pass_out(0, 1)
    pass_in(1)
    pass_out(1, 1)
    ag_first(0)
    loading(5).wait()
    place(5)
    for m in (3, 4, 5):
        start_p1(m)
    pass_out(0, 2)
    ag_second(0)
    own_inner(2)
    begin_hidden(0, 0, 3 * mid)
    pass_out(1, 2)
    own_outer(2)
    ag_far(0)

    all_came((0, 0), (0, 1), (0, 2), (1, 0), (1, 1))
    begin_hidden(0, 3 * mid, PLANE)

    @on_end
    def _():
        for m in (3, 4, 5):
            own_inner(m)

    all_came((1, 2))
    end_hidden(0)
    pass_in(2)
    pass_out(2, 1)

    @on_mid
    def _():
        own_inner(3)

    down(0, 0)
    down(0, 1)
    finish(0, 0)
    for c in range(2, chunks):
        need(0, c)
        down(0, c)
        finish(0, c - 1)
        if c == 3:
            load_merged.wait()
            load_gain2.wait()
        if c >= 3:
            land(0, c - 3)
        if c == 4:
            pass_out(2, 2)
            own_outer(3)
        if c == 5:
            pass_in(3)
            pass_out(3, 1)

            @on_mid
            def _():
                own_inner(4)

    land(0, 5)
    finish(0, 7)
    pass_in(4)

    @on_mid
    def _():
        own_inner(5)

    land(0, 6)
    land(0, 7)
    drain(ag_s.at[0], normed1.at[pl.ds(0, 3), pl.ds(0, half), :])
    drain(rel_s.at[0], normed1.at[pl.ds(0, 3), pl.ds(0, half), :])

    @pl.loop(0, half // step)
    def _(i):
        at = pl.ds(pl.multiple_of(i * step, step), step)
        full = pl.ds(pl.multiple_of(t * half + i * step, step), step)
        scale = lax.rsqrt(jnp.sum(ssq[at, :], axis=-1, keepdims=True) / width + EPS)
        normed2[0, full, :] = (middle[at, :] * scale * gain2[...]).astype(BF16)

    for r, h in ((2, 0), (1, 1), (2, 1), (1, 0)):
        ag(1, r, h).start()
    for h in range(2):
        relay(1, 0, h, t).start()
    pass_out(3, 2)
    own_outer(4)
    pass_in(5)
    pass_out(4, 1)
    ag_first(1)
    pass_out(4, 2)
    own_outer(5)
    ag_second(1)
    pass_out(5, 1)

    drain(sib_s.at[0], sib)
    drain(rs_s.at[0], comb)

    @on_mid
    def _():
        whole_hidden(1, 0, 3)

    all_came((3, 0), (3, 1), (3, 2))
    gate_slots(1, 0, 3 - 3 * mid)
    all_came((4, 0), (4, 1))
    up_slots(1, 0, 3 - 3 * mid)
    ag_far(1)
    @on_mid
    def _():
        whole_hidden(1, 3, 4)

    pass_out(5, 2)

    @on_end
    def _():
        begin_hidden(1, 3, 4)
        came(4, 2).wait_recv()
        end_hidden(1)

    down(1, 0)
    down(1, 1)
    finish(1, 0)
    for c in range(2, chunks):
        need(1, c)
        down(1, c)
        finish(1, c - 1)
        if 3 <= c < chunks - 1:
            land(1, c - 3)
    land(1, chunks - 4)
    land(1, chunks - 3)
    for c in range(chunks - 4):
        store_other(c)
    finish(1, chunks - 1)
    land(1, chunks - 2)
    land(1, chunks - 1)

    for c in range(chunks - 4, chunks):
        store_other(c)
    drain(p1_s.at[0], w.at[:, :, pl.ds(0, (PLANE - 1) * ds)])

    @on_mid
    def _():
        drain(z_s.at[0], w.at[:, :, pl.ds(0, 2 * pw)])
        drain(z_s.at[1], w.at[:, :, pl.ds(0, 3 * pw)])

    @on_end
    def _():
        drain(z_s.at[0], w.at[:, :, pl.ds(0, pw)])

    drain(ag_s.at[0], normed2.at[pl.ds(0, 3), pl.ds(0, half), :])
    drain(rel_s.at[0], normed2.at[:, pl.ds(0, half), :])
    drain(sib_s.at[0], sib)
    drain(rs_s.at[0], comb)
    drain(fin_s.at[0], here)
    pltpu.make_async_copy(tokens, tokens, store.at[0]).wait()


def plane_shards(tokens, merged, gain1, g1, u1, d1, gain2, g2, u2, d2):
    rows, width = tokens.shape
    half = rows // 2
    hid, ds = d1.shape
    q = hid // PLANE
    chunks = LINE * PARTS
    far = pl.BlockSpec(memory_space=pl.ANY)
    dma = lambda *s: pltpu.SemaphoreType.DMA(s)
    return pl.pallas_call(
        kernel,
        out_shape=pltpu.VMEM((rows, width), BF16),
        in_specs=[far] * 10,
        out_specs=far,
        scratch_shapes=[
            pltpu.VMEM((4, ds, hid), BF16),
            pltpu.VMEM((4, hid, ds), BF16),
            pltpu.VMEM((2, hid, ds), BF16),
            pltpu.VMEM((rows, width), BF16),
            pltpu.VMEM((rows, width), BF16),
            pltpu.VMEM((1, width), F32),
            pltpu.VMEM((1, width), F32),
            pltpu.VMEM((half, width), BF16),
            pltpu.VMEM((half, width), BF16),
            pltpu.VMEM((6, q, width), BF16),
            pltpu.VMEM((PLANE, rows, width), BF16),
            pltpu.VMEM((PLANE, rows, width), BF16),
            pltpu.VMEM((PLANE, rows, q), F32),
            pltpu.VMEM((PLANE, rows, q), F32),
            pltpu.VMEM((PLANE, rows, q), BF16),
            pltpu.VMEM((PLANE, rows, width), BF16),
            pltpu.VMEM((PLANE, half, width), BF16),
            pltpu.VMEM((PLANE - 1, half, width), BF16),
            pltpu.VMEM((2, half // 2, width), BF16),
            pltpu.VMEM((2, half, width), BF16),
            pltpu.VMEM((half, width), F32),
            pltpu.VMEM((half, 128), F32),
            dma(10), dma(1), dma(10), dma(2), dma(24 + 2 * (3 * PARTS - 3)),
            dma(1), dma(3, 2), dma(1), dma(PLANE),
            dma(1), dma(2, PLANE), dma(1), dma(chunks, 3),
            dma(1), dma(chunks), dma(1),
        ],
        compiler_params=pltpu.CompilerParams(
            collective_id=0, has_side_effects=True, vmem_limit_bytes=60 * 2**20
        ),
    )(tokens, merged, gain1[None], gain2[None], g1, u1, d1, g2, u2, d2)


def shards(n_fs, n_tp, *args):
    rows, width = args[0].shape
    hid, cols = args[5].shape
    fits = n_fs == PLANE * LINE and n_tp == 2 and cols % 128 == 0 and width % (128 * LINE * PARTS) == 0
    fits = fits and hid % (32 * PLANE) == 0 and rows % 64 == 0
    return plane_shards(*args) if fits else gathered_shards(*args)


def solution(mesh):
    return jax.shard_map(
        functools.partial(shards, mesh.shape["fs"], mesh.shape["tp"]),
        mesh=mesh,
        in_specs=(
            P("fs", None),
            P("fs", None),
            P(),
            P("fs", "tp"),
            P("fs", "tp"),
            P("tp", "fs"),
            P(),
            P("fs", "tp"),
            P("fs", "tp"),
            P("tp", "fs"),
        ),
        out_specs=P("fs", None),
        check_vma=False,
    )
```

```python
import functools

import jax
import jax.numpy as jnp
from jax import lax
from jax.experimental import pallas as pl
from jax.experimental.pallas import tpu as pltpu
from jax.sharding import PartitionSpec as P

EPS = 1e-06
BF16 = jnp.bfloat16
F32 = jnp.float32
PLANE = 4
LINE = 4


def norm_rows(values, gain):
    scale = lax.rsqrt(jnp.mean(values * values, axis=-1, keepdims=True) + EPS)
    return values * scale * gain


def gathered_block(normed, gate, up, down):
    gate_whole = lax.all_gather(gate, "fs", axis=0, tiled=True)
    up_whole = lax.all_gather(up, "fs", axis=0, tiled=True)
    g = jnp.dot(normed, gate_whole, preferred_element_type=F32)
    u = jnp.dot(normed, up_whole, preferred_element_type=F32)
    hidden = (jax.nn.silu(g) * u).astype(BF16)
    down_whole = lax.all_gather(down, "fs", axis=1, tiled=True)
    part = jnp.dot(hidden, down_whole, preferred_element_type=F32)
    return lax.psum(part.astype(BF16), "tp").astype(F32)


def gathered_shards(tokens, merged, gain1, g1, u1, d1, gain2, g2, u2, d2):
    source = tokens.astype(F32)
    middle = source + merged.astype(F32)
    normed = norm_rows(source, gain1).astype(BF16)
    middle = middle + 0.5 * gathered_block(normed, g1, u1, d1)
    normed = norm_rows(middle, gain2).astype(BF16)
    return (middle + 0.5 * gathered_block(normed, g2, u2, d2)).astype(BF16)


def kernel(
    tokens_h, merged_h, gain1_h, gain2_h, wa, wb, wc, wd, we, wf, out_h,
    raw, turned, straight, tokens, merged, gain1, gain2, here, fin, w, normed1, normed2, acc_g, acc_u, hidden,
    prod, sib, comb, diag, rsr, middle, ssq,
    load, p1_s, p1_r, z_s, z_r,
    ag_s, ag_r, rel_s, rel_r, sib_s, sib_r, rs_s, rs_r, fin_s, fin_r, store,
):
    weights_in = (wa, wb, wc, wd, we, wf)
    fs = lax.axis_index("fs")
    t = lax.axis_index("tp")
    z = fs // PLANE
    p = fs % PLANE
    rows, width = tokens.shape
    half = rows // 2
    quarter = half // 2
    q, pw = w.shape[1], width // LINE
    ds = wc.shape[1]
    step = 16

    def dev(zz, pp, tt):
        return {"fs": zz * PLANE + pp, "tp": tt}

    peers = (p, p + 1 - 2 * (p % 2), (p + 2) % PLANE, PLANE - 1 - p)
    to_peer = [dev(z, pp, t) for pp in peers]
    sibling = dev(z, p, 1 - t)

    low = (z < 2).astype(jnp.int32)
    toward = 2 * low - 1
    mid = (z % 3 != 0).astype(jnp.int32)
    zi, zo = z + toward, z - toward * mid
    inner, outer = dev(zi, p, t), dev(zo, p, t)

    def on_mid(f):
        pl.when(mid == 1)(f)

    def on_end(f):
        pl.when(mid == 0)(f)

    HALVES = ((0, pw // 2), (pw // 2, pw // 2))
    LAST = ((0, pw // 2), (pw // 2, pw // 4), (3 * pw // 4, pw // 4))

    def remote(src, dst, s, r, to):
        return pltpu.make_async_remote_copy(
            src_ref=src, dst_ref=dst, send_sem=s, recv_sem=r,
            device_id=to, device_id_type=pl.DeviceIdType.MESH,
        )

    mine = pl.ds(pl.multiple_of(t * half, 16), half)
    other = pl.ds(pl.multiple_of((1 - t) * half, 16), half)

    def shard_of(m):
        k = m // 3
        return straight.at[k] if m % 3 == 2 else turned.at[2 * k + m % 3]

    def loading(m):
        k = m // 3
        return pltpu.make_async_copy(
            weights_in[m], straight.at[k] if m % 3 == 2 else raw.at[2 * k + m % 3], load.at[m]
        )

    load_tokens = pltpu.make_async_copy(tokens_h, tokens, load.at[6])
    load_merged = pltpu.make_async_copy(merged_h, merged, load.at[7])
    load_gain1 = pltpu.make_async_copy(gain1_h, gain1, load.at[8])
    load_gain2 = pltpu.make_async_copy(gain2_h, gain2, load.at[9])
    for m in (0, 1):
        loading(m).start()
    load_tokens.start()
    load_gain1.start()
    for m in (3, 4, 2, 5):
        loading(m).start()
    load_merged.start()
    load_gain2.start()

    barrier = pltpu.get_barrier_semaphore()
    targets = [inner, sibling] + to_peer[1:]
    for to in targets:
        pl.semaphore_signal(barrier, inc=1, device_id=to, device_id_type=pl.DeviceIdType.MESH)

    @on_mid
    def _():
        pl.semaphore_signal(barrier, inc=1, device_id=outer, device_id_type=pl.DeviceIdType.MESH)

    def turn(m):
        k = 2 * (m // 3) + m % 3
        loading(m).wait()
        for j in range(raw.shape[2] // 128):
            turned[k, j * 128:(j + 1) * 128, :] = raw[k, :, j * 128:(j + 1) * 128].T

    def lanes_of(zz, pp):
        return pl.ds(pl.multiple_of((zz * PLANE + pp) * ds, ds), ds)

    def p1_sem(m, r):
        return p1_r.at[3 * m + r - 1 if m < 2 else 4 + m]

    def p1(m, r):
        src = shard_of(m).at[pl.ds(pl.multiple_of(peers[r] * q, 16), q), :]
        return remote(src, w.at[m, :, lanes_of(z, p)], p1_s.at[0], p1_sem(m, r), to_peer[r])

    def p1_in(m, r):
        src = w.at[m, :, lanes_of(z, peers[r])]
        return remote(src, src, p1_s.at[0], p1_sem(m, r), to_peer[r])

    def p1_whole(m):
        src = w.at[m, :, pl.ds(0, (PLANE - 1) * ds)]
        return remote(src, src, p1_s.at[0], p1_sem(m, 1), to_peer[1])

    def place(m):
        w[m, :, lanes_of(z, p)] = shard_of(m)[pl.ds(pl.multiple_of(p * q, 16), q), :]

    def start_p1(m):
        for r in (3, 1, 2):
            p1(m, r).start()

    def blk(m, zz):
        return w.at[m, :, pl.ds(pl.multiple_of(zz * pw, pw), pw)]

    first_slot = 3 * (1 - mid)
    def z_sem(m, slot):
        return z_r.at[(0, 4, 9, 16, 20, 25)[m] + slot]

    def to_inner(m, r=None):
        at = blk(m, z) if r is None else w.at[m, :, lanes_of(z, peers[r])]
        return remote(at, at, z_s.at[0], z_sem(m, first_slot), inner)

    def to_outer(m, r):
        at = w.at[m, :, lanes_of(z, peers[r])]
        return remote(at, at, z_s.at[1], z_sem(m, 0), outer)

    def on_inner(m):
        return remote(blk(m, zo), blk(m, zo), z_s.at[0], z_sem(m, 1), inner)

    def cuts(m, d):
        if m % 3 == 1 and d == 2:
            return HALVES
        if m % 3 < 2:
            return ((0, pw),)
        if m == 5 and d == 2:
            return LAST
        return HALVES

    def outward(m, d, k):
        lo, n = cuts(m, d)[k]
        at = w.at[m, :, pl.ds(pl.multiple_of((z + d * toward) * pw + lo, 128), n)]
        return remote(at, at, z_s.at[1], z_sem(m, (d, 4 + d if m % 3 == 2 else 4, 7)[k]), outer)

    early = (0, 1, 3, 4)

    def came(m, slot):
        zz = zo if slot == 3 else z + (slot + 1) * toward
        return remote(blk(m, zz), blk(m, zz), z_s.at[0], z_sem(m, slot), inner)

    def came_part(m, slot, k):
        lo, n = cuts(m, slot)[k]
        at = w.at[m, :, pl.ds(pl.multiple_of((z + (slot + 1) * toward) * pw + lo, 128), n)]
        return remote(at, at, z_s.at[0], z_sem(m, (slot, 4 + slot if m % 3 == 2 else 4, 7)[k]), inner)

    def piece_out(m, r):
        to_inner(m, r).start()

        @on_mid
        def _():
            to_outer(m, r).start()

    def own_now(m):
        for r in (1, 2, 3):
            p1_in(m, r).wait_recv()
            piece_out(m, r)

    def own_inner(m):
        p1_whole(m).wait_recv()
        if m in early:
            @pl.when(t == 0)
            def _():
                for r in (1, 2, 3):
                    to_inner(m, r).start()

            @pl.when(t == 1)
            def _():
                to_inner(m).start()
        else:
            to_inner(m).start()

    def own_outer(m):
        @on_mid
        def _():
            if m in early:
                @pl.when(t == 0)
                def _():
                    for r in (1, 2, 3):
                        to_outer(m, r).start()

                @pl.when(t == 1)
                def _():
                    outward(m, 0, 0).start()
            else:
                for k in range(len(cuts(m, 0))):
                    outward(m, 0, k).start()

    def pass_in(m):
        @on_mid
        def _():
            came(m, 3).wait_recv()
            on_inner(m).start()

    def pass_out(m, d):
        @on_mid
        def _():
            came(m, d - 1).wait_recv()
            for k in range(len(cuts(m, d))):
                outward(m, d, k).start()

    def need(f, c):
        block, k = table[f][c]
        if block:
            @on_end
            def _():
                came_part(3 * f + 2, block - 1, k).wait_recv()

    def drain(sem, ref):
        remote(ref, ref, sem, sem, sibling).wait_send()

    bufs = (normed1, normed2)

    def piece(tt, h):
        return pl.ds(pl.multiple_of(tt * half + h * quarter, 16), quarter)

    def ag(f, r, h):
        at = piece(t, h)
        return remote(bufs[f].at[0, at, :], bufs[f].at[r, at, :], ag_s.at[0], ag_r.at[r - 1, h], to_peer[r])

    def ag_on(f, h):
        at = piece(t, h)
        return remote(bufs[f].at[2 - h, at, :], bufs[f].at[3, at, :], ag_s.at[0], ag_r.at[2, h], to_peer[1 + h])

    def relay(f, r, h, tt):
        at = bufs[f].at[r, piece(tt, h), :]
        return remote(at, at, rel_s.at[0], rel_r.at[r], sibling)

    def ag_first(f):
        for r, h in ((2, 0), (1, 1)):
            ag(f, r, h).wait_recv()
            ag_on(f, h).start()
            relay(f, r, h, t).start()

    def ag_second(f):
        for r, h in ((2, 1), (1, 0)):
            ag(f, r, h).wait_recv()
            relay(f, r, h, t).start()

    def ag_far(f):
        for h in range(2):
            ag_on(f, h).wait_recv()
            relay(f, 3, h, t).start()

    zs = (z, zi, jnp.where(mid == 1, zo, z + 2 * toward), jnp.where(mid == 1, z + 2 * toward, z + 3 * toward))
    table = [[(b, k) for b in range(LINE) for k in range(len(cuts(3 * f + 2, b - 1)))] for f in range(2)]
    sizes = [[cuts(3 * f + 2, b - 1)[k] for b, k in table[f]] for f in range(2)]
    lanes = [
        [pl.ds(pl.multiple_of(zs[b] * pw + lo, 128), n) for (b, k), (lo, n) in zip(table[f], sizes[f])]
        for f in range(2)
    ]
    lanes_a = pl.ds(pl.multiple_of((1 - low) * pw, pw), 3 * pw)
    lanes_b = [pl.ds(pl.multiple_of(low * 3 * pw + lo, 128), n) for lo, n in HALVES]
    first, second = pl.ds(0, quarter), pl.ds(quarter, quarter)

    def to_sibling(f, c, r):
        return remote(prod.at[r, other, lanes[f][c]], sib.at[r, :, lanes[f][c]], sib_s.at[0], sib_r.at[c % 3, r], sibling)

    def rs(f, c, kind):
        at = lanes[f][c]
        src, dst, r = (
            (comb.at[2, first, at], diag.at[0, :, at], 1),
            (comb.at[2, second, at], diag.at[1, :, at], 2),
            (comb.at[0, first, at], rsr.at[0, first, at], 1),
            (comb.at[0, second, at], rsr.at[0, second, at], 1),
            (comb.at[1, second, at], rsr.at[1, second, at], 2),
            (comb.at[1, first, at], rsr.at[1, first, at], 2),
        )[kind]
        return remote(src, dst, rs_s.at[0], rs_r.at[c, min(kind, 2)], to_peer[r])

    def product(f, k, r, at):
        dims = (((1,), (1,)), ((), ()))
        return lax.dot_general(bufs[f][r, :, at], w[3 * f + k, :, at], dims, preferred_element_type=F32)

    def slot_in(f, r):
        @pl.when(r > (0 if f == 0 else -1))
        def _():
            at = bufs[f].at[r, other, :]
            remote(at, at, rel_s.at[0], rel_r.at[r], sibling).wait_recv()

    def silu(g):
        return g / (1.0 + jnp.exp(-g))

    every = slice(None)

    def gate_slots(f, lo, hi):
        @pl.loop(lo, hi)
        def _(r):
            slot_in(f, r)
            acc_g[r] = silu(product(f, 0, r, every))

    def up_slots(f, lo, hi):
        @pl.loop(lo, hi)
        def _(r):
            acc_u[r] = product(f, 1, r, lanes_a)

    def begin_hidden(f, lo, hi):
        @pl.loop(lo, hi)
        def _(r):
            slot_in(f, r)
            acc_g[r] = silu(product(f, 0, r, every))
            acc_u[r] = product(f, 1, r, lanes_a)

    def first_product(f, r):
        prod[r, :, lanes[f][0]] = jnp.dot(hidden[r], w[3 * f + 2, :, lanes[f][0]], preferred_element_type=F32).astype(BF16)
        to_sibling(f, 0, r).start()

    def more_hidden(f):
        @pl.loop(0, PLANE)
        def _(r):
            acc_u[r] = acc_u[r] + product(f, 1, r, lanes_b[0])

    def end_hidden(f):
        @pl.loop(0, PLANE)
        def _(k):
            r = PLANE - 1 - k
            u = acc_u[r] + product(f, 1, r, lanes_b[1])
            hidden[r] = (acc_g[r] * u).astype(BF16)
            first_product(f, r)

    def whole_hidden(f, lo, hi):
        @pl.loop(lo, hi)
        def _(r):
            slot_in(f, r)
            g = silu(product(f, 0, r, every))
            hidden[r] = (g * product(f, 1, r, every)).astype(BF16)
            first_product(f, r)

    def all_came(*pairs):
        @on_end
        def _():
            for m, slot in pairs:
                came(m, slot).wait_recv()

    def combine(f, c, r):
        at = lanes[f][c]
        to_sibling(f, c, r).wait_recv()

        @pl.loop(0, half // (2 * step))
        def _(i):
            some = pl.ds(pl.multiple_of(i * 2 * step, step), 2 * step)
            full = pl.ds(pl.multiple_of(t * half + i * 2 * step, step), 2 * step)
            comb[r - 1, some, at] = (prod[r, full, at].astype(F32) + sib[r, some, at].astype(F32)).astype(BF16)

        for kind in (None, (2,), (4,), (0, 1))[r]:
            rs(f, c, kind).start()

    def combine_all(f, c):
        for r in (3, 2, 1):
            combine(f, c, r)
        to_sibling(f, c, 0).wait_recv()

    def produce(f, c):
        at = lanes[f][c]

        @pl.loop(0, PLANE)
        def _(k):
            r = PLANE - 1 - k
            prod[r, :, at] = jnp.dot(hidden[r], w[3 * f + 2, :, at], preferred_element_type=F32).astype(BF16)
            to_sibling(f, c, r).start()

    def down(f, c):
        produce(f, c)
        combine_all(f, c)

    def finish(f, c):
        at = lanes[f][c]
        rs(f, c, 0).wait_recv()
        comb[1, first, at] = (comb[1, first, at].astype(F32) + diag[0, :, at].astype(F32)).astype(BF16)
        rs(f, c, 5).start()
        rs(f, c, 1).wait_recv()
        comb[0, second, at] = (comb[0, second, at].astype(F32) + diag[1, :, at].astype(F32)).astype(BF16)
        rs(f, c, 3).start()

    def reduced(rows_at, full, at):
        total = prod[0, full, at].astype(F32) + sib[0, rows_at, at].astype(F32)
        return total + rsr[0, rows_at, at].astype(F32) + rsr[1, rows_at, at].astype(F32)

    def out_across(c):
        at = lanes[1][c]
        return remote(here.at[:, at], fin.at[:, at], fin_s.at[0], fin_r.at[c], sibling)

    def out_store(c, k):
        at = lanes[1][c]
        return pltpu.make_async_copy((here, fin)[k].at[:, at], out_h.at[(mine, other)[k], at], store.at[0])

    def store_other(c):
        out_across(c).wait_recv()
        out_store(c, 1).start()

    def land(f, c):
        at = lanes[f][c]
        remote(rsr.at[:, :, at], rsr.at[:, :, at], rs_s.at[0], rs_r.at[c, 2], sibling).wait_recv()

        @pl.loop(0, half // (2 * step))
        def _(i):
            some = pl.ds(pl.multiple_of(i * 2 * step, step), 2 * step)
            full = pl.ds(pl.multiple_of(t * half + i * 2 * step, step), 2 * step)
            if f == 0:
                value = tokens[full, at].astype(F32) + merged[full, at].astype(F32) + 0.5 * reduced(some, full, at)
                middle[some, at] = value
                squares = value * value
                sums = sum(squares[:, k * 128:(k + 1) * 128] for k in range(sizes[f][c][1] // 128))
                ssq[some, :] = sums if c == 0 else ssq[some, :] + sums
            else:
                here[some, at] = (middle[some, at] + 0.5 * reduced(some, full, at)).astype(BF16)

        if f == 1:
            out_across(c).start()
            out_store(c, 0).start()

    def norm_first(start, count):
        @pl.loop(0, count // step)
        def _(i):
            at = pl.ds(pl.multiple_of(start + i * step, step), step)
            normed1[0, at, :] = norm_rows(tokens[at, :].astype(F32), gain1[...]).astype(BF16)

    turn(0)
    place(0)
    pl.semaphore_wait(barrier, len(targets) + mid)
    start_p1(0)
    piece_out(0, 0)
    turn(1)
    start_p1(1)
    place(1)
    piece_out(1, 0)
    for m in (3, 4):
        turn(m)
        place(m)

    @pl.when(t == 0)
    def _():
        for m in (3, 4):
            piece_out(m, 0)

    load_tokens.wait()
    load_gain1.wait()
    norm_first(t * half, half)
    for r, h in ((2, 0), (1, 1), (2, 1), (1, 0)):
        ag(0, r, h).start()
    loading(2).wait()
    start_p1(2)
    place(2)
    own_now(0)
    norm_first((1 - t) * half, half)
    own_now(1)
    pass_in(0)
    pass_out(0, 1)
    pass_in(1)
    pass_out(1, 1)
    ag_first(0)
    loading(5).wait()
    place(5)
    for m in (3, 4, 5):
        start_p1(m)
    pass_out(0, 2)
    ag_second(0)
    own_inner(2)
    begin_hidden(0, 0, 3 * mid)
    pass_out(1, 2)
    own_outer(2)
    ag_far(0)

    all_came((0, 0), (0, 1), (0, 2), (1, 0), (1, 1))
    begin_hidden(0, 3 * mid, PLANE)

    @on_end
    def _():
        for m in (3, 4, 5):
            own_inner(m)

    @on_end
    def _():
        came_part(1, 2, 0).wait_recv()

    more_hidden(0)

    @on_end
    def _():
        came_part(1, 2, 1).wait_recv()

    end_hidden(0)
    combine_all(0, 0)
    pass_in(2)
    pass_out(2, 1)

    @on_mid
    def _():
        own_inner(3)

    down(0, 1)
    finish(0, 0)
    for c in range(2, len(table[0])):
        need(0, c)
        down(0, c)
        finish(0, c - 1)
        if c == 3:
            load_merged.wait()
            load_gain2.wait()
        if c >= 3:
            land(0, c - 3)
        if c == 4:
            pass_out(2, 2)
            own_outer(3)
        if c == 5:
            pass_in(3)
            pass_out(3, 1)

            @on_mid
            def _():
                own_inner(4)

    land(0, 5)
    finish(0, 7)
    pass_in(4)

    @on_mid
    def _():
        own_inner(5)

    land(0, 6)
    land(0, 7)
    drain(ag_s.at[0], normed1.at[pl.ds(0, 3), pl.ds(0, half), :])
    drain(rel_s.at[0], normed1.at[pl.ds(0, 3), pl.ds(0, half), :])

    @pl.loop(0, half // step)
    def _(i):
        at = pl.ds(pl.multiple_of(i * step, step), step)
        full = pl.ds(pl.multiple_of(t * half + i * step, step), step)
        scale = lax.rsqrt(jnp.sum(ssq[at, :], axis=-1, keepdims=True) / width + EPS)
        normed2[0, full, :] = (middle[at, :] * scale * gain2[...]).astype(BF16)

    for r, h in ((2, 0), (1, 1), (2, 1), (1, 0)):
        ag(1, r, h).start()
    for h in range(2):
        relay(1, 0, h, t).start()
    pass_out(3, 2)
    own_outer(4)
    pass_in(5)
    pass_out(4, 1)
    ag_first(1)
    pass_out(4, 2)
    own_outer(5)
    ag_second(1)
    pass_out(5, 1)

    drain(sib_s.at[0], sib)
    drain(rs_s.at[0], comb)

    @on_mid
    def _():
        whole_hidden(1, 0, 3)

    all_came((3, 0), (3, 1), (3, 2))
    gate_slots(1, 0, 3 - 3 * mid)
    all_came((4, 0), (4, 1))
    up_slots(1, 0, 3 - 3 * mid)
    ag_far(1)
    @on_mid
    def _():
        whole_hidden(1, 3, 4)
        combine_all(1, 0)

    pass_out(5, 2)

    @on_end
    def _():
        begin_hidden(1, 3, 4)
        came_part(4, 2, 0).wait_recv()
        more_hidden(1)
        came_part(4, 2, 1).wait_recv()
        end_hidden(1)
        combine_all(1, 0)

    chunks = len(table[1])
    down(1, 1)
    finish(1, 0)
    for c in range(2, chunks - 2):
        need(1, c)
        down(1, c)
        finish(1, c - 1)
        if c >= 3:
            land(1, c - 3)
    need(1, chunks - 2)
    produce(1, chunks - 2)
    need(1, chunks - 1)
    produce(1, chunks - 1)
    combine_all(1, chunks - 2)
    combine_all(1, chunks - 1)
    finish(1, chunks - 3)
    finish(1, chunks - 2)
    land(1, chunks - 5)
    land(1, chunks - 4)
    for c in range(chunks - 4):
        store_other(c)
    finish(1, chunks - 1)
    land(1, chunks - 3)
    land(1, chunks - 2)
    land(1, chunks - 1)

    for c in range(chunks - 4, chunks):
        store_other(c)
    drain(p1_s.at[0], w.at[:, :, pl.ds(0, (PLANE - 1) * ds)])

    @on_mid
    def _():
        drain(z_s.at[0], w.at[:, :, pl.ds(0, 2 * pw)])
        drain(z_s.at[1], w.at[:, :, pl.ds(0, 3 * pw)])

    @on_end
    def _():
        drain(z_s.at[0], w.at[:, :, pl.ds(0, pw)])

    drain(ag_s.at[0], normed2.at[pl.ds(0, 3), pl.ds(0, half), :])
    drain(rel_s.at[0], normed2.at[:, pl.ds(0, half), :])
    drain(sib_s.at[0], sib)
    drain(rs_s.at[0], comb)
    drain(fin_s.at[0], here)
    pltpu.make_async_copy(tokens, tokens, store.at[0]).wait()


def plane_shards(tokens, merged, gain1, g1, u1, d1, gain2, g2, u2, d2):
    rows, width = tokens.shape
    half = rows // 2
    hid, ds = d1.shape
    q = hid // PLANE
    chunks = 2 * LINE + 1
    far = pl.BlockSpec(memory_space=pl.ANY)
    dma = lambda *s: pltpu.SemaphoreType.DMA(s)
    return pl.pallas_call(
        kernel,
        out_shape=pltpu.VMEM((rows, width), BF16),
        in_specs=[far] * 10,
        out_specs=far,
        scratch_shapes=[
            pltpu.VMEM((4, ds, hid), BF16),
            pltpu.VMEM((4, hid, ds), BF16),
            pltpu.VMEM((2, hid, ds), BF16),
            pltpu.VMEM((rows, width), BF16),
            pltpu.VMEM((rows, width), BF16),
            pltpu.VMEM((1, width), F32),
            pltpu.VMEM((1, width), F32),
            pltpu.VMEM((half, width), BF16),
            pltpu.VMEM((half, width), BF16),
            pltpu.VMEM((6, q, width), BF16),
            pltpu.VMEM((PLANE, rows, width), BF16),
            pltpu.VMEM((PLANE, rows, width), BF16),
            pltpu.VMEM((PLANE, rows, q), F32),
            pltpu.VMEM((PLANE, rows, q), F32),
            pltpu.VMEM((PLANE, rows, q), BF16),
            pltpu.VMEM((PLANE, rows, width), BF16),
            pltpu.VMEM((PLANE, half, width), BF16),
            pltpu.VMEM((PLANE - 1, half, width), BF16),
            pltpu.VMEM((2, half // 2, width), BF16),
            pltpu.VMEM((2, half, width), BF16),
            pltpu.VMEM((half, width), F32),
            pltpu.VMEM((half, 128), F32),
            dma(10), dma(1), dma(10), dma(2), dma(33),
            dma(1), dma(3, 2), dma(1), dma(PLANE),
            dma(1), dma(3, PLANE), dma(1), dma(chunks, 3),
            dma(1), dma(chunks), dma(1),
        ],
        compiler_params=pltpu.CompilerParams(
            collective_id=0, has_side_effects=True, vmem_limit_bytes=60 * 2**20
        ),
    )(tokens, merged, gain1[None], gain2[None], g1, u1, d1, g2, u2, d2)


def shards(n_fs, n_tp, *args):
    rows, width = args[0].shape
    hid, cols = args[5].shape
    fits = n_fs == PLANE * LINE and n_tp == 2 and cols % 128 == 0 and width % (512 * LINE) == 0
    fits = fits and hid % (32 * PLANE) == 0 and rows % 64 == 0
    return plane_shards(*args) if fits else gathered_shards(*args)


def solution(mesh):
    return jax.shard_map(
        functools.partial(shards, mesh.shape["fs"], mesh.shape["tp"]),
        mesh=mesh,
        in_specs=(
            P("fs", None),
            P("fs", None),
            P(),
            P("fs", "tp"),
            P("fs", "tp"),
            P("tp", "fs"),
            P(),
            P("fs", "tp"),
            P("fs", "tp"),
            P("tp", "fs"),
        ),
        out_specs=P("fs", None),
        check_vma=False,
    )
```

```python
import functools

import jax
import jax.numpy as jnp
from jax import lax
from jax.experimental import pallas as pl
from jax.experimental.pallas import tpu as pltpu
from jax.sharding import PartitionSpec as P

EPS = 1e-06
BF16 = jnp.bfloat16
F32 = jnp.float32
PLANE = 4
LINE = 4


def norm_rows(values, gain):
    scale = lax.rsqrt(jnp.mean(values * values, axis=-1, keepdims=True) + EPS)
    return values * scale * gain


def gathered_block(normed, gate, up, down):
    gate_whole = lax.all_gather(gate, "fs", axis=0, tiled=True)
    up_whole = lax.all_gather(up, "fs", axis=0, tiled=True)
    g = jnp.dot(normed, gate_whole, preferred_element_type=F32)
    u = jnp.dot(normed, up_whole, preferred_element_type=F32)
    hidden = (jax.nn.silu(g) * u).astype(BF16)
    down_whole = lax.all_gather(down, "fs", axis=1, tiled=True)
    part = jnp.dot(hidden, down_whole, preferred_element_type=F32)
    return lax.psum(part.astype(BF16), "tp").astype(F32)


def gathered_shards(tokens, merged, gain1, g1, u1, d1, gain2, g2, u2, d2):
    source = tokens.astype(F32)
    middle = source + merged.astype(F32)
    normed = norm_rows(source, gain1).astype(BF16)
    middle = middle + 0.5 * gathered_block(normed, g1, u1, d1)
    normed = norm_rows(middle, gain2).astype(BF16)
    return (middle + 0.5 * gathered_block(normed, g2, u2, d2)).astype(BF16)


def kernel(
    tokens_h, merged_h, gain1_h, gain2_h, wa, wb, wc, wd, we, wf, out_h,
    raw, turned, straight, tokens, merged, gain1, gain2, here, fin, w, normed1, normed2, acc_g, acc_u, hidden,
    prod, sib, comb, diag, rsr, middle, ssq,
    load, p1_s, p1_r, z_s, z_r,
    ag_s, ag_r, rel_s, rel_r, sib_s, sib_r, rs_s, rs_r, fin_s, fin_r, store,
):
    weights_in = (wa, wb, wc, wd, we, wf)
    fs = lax.axis_index("fs")
    t = lax.axis_index("tp")
    z = fs // PLANE
    p = fs % PLANE
    rows, width = tokens.shape
    half = rows // 2
    quarter = half // 2
    q, pw = w.shape[1], width // LINE
    ds = wc.shape[1]
    step = 16

    def dev(zz, pp, tt):
        return {"fs": zz * PLANE + pp, "tp": tt}

    peers = (p, p + 1 - 2 * (p % 2), (p + 2) % PLANE, PLANE - 1 - p)
    to_peer = [dev(z, pp, t) for pp in peers]
    sibling = dev(z, p, 1 - t)

    low = (z < 2).astype(jnp.int32)
    toward = 2 * low - 1
    mid = (z % 3 != 0).astype(jnp.int32)
    zi, zo = z + toward, z - toward * mid
    inner, outer = dev(zi, p, t), dev(zo, p, t)

    def on_mid(f):
        pl.when(mid == 1)(f)

    def on_end(f):
        pl.when(mid == 0)(f)

    HALVES = ((0, pw // 2), (pw // 2, pw // 2))
    LAST = ((0, pw // 2), (pw // 2, pw // 4), (3 * pw // 4, pw // 4))

    def remote(src, dst, s, r, to):
        return pltpu.make_async_remote_copy(
            src_ref=src, dst_ref=dst, send_sem=s, recv_sem=r,
            device_id=to, device_id_type=pl.DeviceIdType.MESH,
        )

    mine = pl.ds(pl.multiple_of(t * half, 16), half)
    other = pl.ds(pl.multiple_of((1 - t) * half, 16), half)

    def shard_of(m):
        k = m // 3
        return straight.at[k] if m % 3 == 2 else turned.at[2 * k + m % 3]

    def loading(m):
        k = m // 3
        return pltpu.make_async_copy(
            weights_in[m], straight.at[k] if m % 3 == 2 else raw.at[2 * k + m % 3], load.at[m]
        )

    load_tokens = pltpu.make_async_copy(tokens_h, tokens, load.at[6])
    load_merged = pltpu.make_async_copy(merged_h, merged, load.at[7])
    load_gain1 = pltpu.make_async_copy(gain1_h, gain1, load.at[8])
    load_gain2 = pltpu.make_async_copy(gain2_h, gain2, load.at[9])
    for m in (0, 1):
        loading(m).start()
    load_tokens.start()
    load_gain1.start()
    for m in (3, 4, 2, 5):
        loading(m).start()
    load_merged.start()
    load_gain2.start()

    barrier = pltpu.get_barrier_semaphore()
    targets = [inner, sibling] + to_peer[1:]
    for to in targets:
        pl.semaphore_signal(barrier, inc=1, device_id=to, device_id_type=pl.DeviceIdType.MESH)

    @on_mid
    def _():
        pl.semaphore_signal(barrier, inc=1, device_id=outer, device_id_type=pl.DeviceIdType.MESH)

    def turn(m):
        k = 2 * (m // 3) + m % 3
        loading(m).wait()
        for j in range(raw.shape[2] // 128):
            turned[k, j * 128:(j + 1) * 128, :] = raw[k, :, j * 128:(j + 1) * 128].T

    def lanes_of(zz, pp):
        return pl.ds(pl.multiple_of((zz * PLANE + pp) * ds, ds), ds)

    def p1_sem(m, r):
        return p1_r.at[3 * m + r - 1 if m < 2 else 4 + m]

    def p1(m, r):
        src = shard_of(m).at[pl.ds(pl.multiple_of(peers[r] * q, 16), q), :]
        return remote(src, w.at[m, :, lanes_of(z, p)], p1_s.at[0], p1_sem(m, r), to_peer[r])

    def p1_in(m, r):
        src = w.at[m, :, lanes_of(z, peers[r])]
        return remote(src, src, p1_s.at[0], p1_sem(m, r), to_peer[r])

    def p1_whole(m):
        src = w.at[m, :, pl.ds(0, (PLANE - 1) * ds)]
        return remote(src, src, p1_s.at[0], p1_sem(m, 1), to_peer[1])

    def place(m):
        w[m, :, lanes_of(z, p)] = shard_of(m)[pl.ds(pl.multiple_of(p * q, 16), q), :]

    def start_p1(m):
        for r in (3, 1, 2):
            p1(m, r).start()

    def blk(m, zz):
        return w.at[m, :, pl.ds(pl.multiple_of(zz * pw, pw), pw)]

    first_slot = 2 * (1 - mid)
    def z_sem(m, slot):
        return z_r.at[(0, 3, 7, 13, 16, 20)[m] + slot]

    def to_inner(m, r=None):
        at = blk(m, z) if r is None else w.at[m, :, lanes_of(z, peers[r])]
        return remote(at, at, z_s.at[0], z_sem(m, first_slot), inner)

    def to_outer(m, r):
        at = w.at[m, :, lanes_of(z, peers[r])]
        return remote(at, at, z_s.at[1], z_sem(m, 0), outer)

    def on_inner(m):
        return remote(blk(m, zo), blk(m, zo), z_s.at[0], z_sem(m, 1), inner)

    def cuts(m, d):
        if m % 3 == 1 and d == 2:
            return HALVES
        if m % 3 < 2:
            return ((0, pw),)
        if m == 5 and d == 2:
            return LAST
        return HALVES

    def outward(m, d, k):
        lo, n = cuts(m, d)[k]
        at = w.at[m, :, pl.ds(pl.multiple_of((z + d * toward) * pw + lo, 128), n)]
        return remote(at, at, z_s.at[1], z_sem(m, (d, 3 + d if m % 3 == 2 else 3, 6)[k]), outer)

    early = (0, 1, 3, 4)

    def came(m, slot):
        zz = zo if slot == 3 else z + (slot + 1) * toward
        return remote(blk(m, zz), blk(m, zz), z_s.at[0], z_sem(m, min(slot, 2)), inner)

    def came_part(m, slot, k):
        lo, n = cuts(m, slot)[k]
        at = w.at[m, :, pl.ds(pl.multiple_of((z + (slot + 1) * toward) * pw + lo, 128), n)]
        return remote(at, at, z_s.at[0], z_sem(m, (slot, 3 + slot if m % 3 == 2 else 3, 6)[k]), inner)

    def piece_out(m, r):
        to_inner(m, r).start()

        @on_mid
        def _():
            to_outer(m, r).start()

    def own_now(m):
        for r in (1, 2, 3):
            p1_in(m, r).wait_recv()
            piece_out(m, r)

    def own_inner(m):
        p1_whole(m).wait_recv()
        if m in early:
            @pl.when(t == 0)
            def _():
                for r in (1, 2, 3):
                    to_inner(m, r).start()

            @pl.when(t == 1)
            def _():
                to_inner(m).start()
        else:
            to_inner(m).start()

    def own_outer(m):
        @on_mid
        def _():
            if m in early:
                @pl.when(t == 0)
                def _():
                    for r in (1, 2, 3):
                        to_outer(m, r).start()

                @pl.when(t == 1)
                def _():
                    outward(m, 0, 0).start()
            else:
                for k in range(len(cuts(m, 0))):
                    outward(m, 0, k).start()

    def pass_in(m):
        @on_mid
        def _():
            came(m, 3).wait_recv()
            on_inner(m).start()

    def pass_out(m, d):
        @on_mid
        def _():
            came(m, d - 1).wait_recv()
            for k in range(len(cuts(m, d))):
                outward(m, d, k).start()

    def need(f, c):
        block, k = table[f][c]
        if block:
            @on_end
            def _():
                came_part(3 * f + 2, block - 1, k).wait_recv()

    def drain(sem, ref):
        remote(ref, ref, sem, sem, sibling).wait_send()

    bufs = (normed1, normed2)

    def piece(tt, h):
        return pl.ds(pl.multiple_of(tt * half + h * quarter, 16), quarter)

    def ag(f, r, h):
        at = piece(t, h)
        return remote(bufs[f].at[0, at, :], bufs[f].at[r, at, :], ag_s.at[0], ag_r.at[r - 1, h], to_peer[r])

    def ag_on(f, h):
        at = piece(t, h)
        return remote(bufs[f].at[2 - h, at, :], bufs[f].at[3, at, :], ag_s.at[0], ag_r.at[2, h], to_peer[1 + h])

    def relay(f, r, h, tt):
        at = bufs[f].at[r, piece(tt, h), :]
        return remote(at, at, rel_s.at[0], rel_r.at[r], sibling)

    def ag_first(f):
        for r, h in ((2, 0), (1, 1)):
            ag(f, r, h).wait_recv()
            ag_on(f, h).start()
            relay(f, r, h, t).start()

    def ag_second(f):
        for r, h in ((2, 1), (1, 0)):
            ag(f, r, h).wait_recv()
            relay(f, r, h, t).start()

    def ag_far(f):
        for h in range(2):
            ag_on(f, h).wait_recv()
            relay(f, 3, h, t).start()

    zs = (z, zi, jnp.where(mid == 1, zo, z + 2 * toward), jnp.where(mid == 1, z + 2 * toward, z + 3 * toward))
    table = [[(b, k) for b in range(LINE) for k in range(len(cuts(3 * f + 2, b - 1)))] for f in range(2)]
    sizes = [[cuts(3 * f + 2, b - 1)[k] for b, k in table[f]] for f in range(2)]
    lanes = [
        [pl.ds(pl.multiple_of(zs[b] * pw + lo, 128), n) for (b, k), (lo, n) in zip(table[f], sizes[f])]
        for f in range(2)
    ]
    lanes_a = pl.ds(pl.multiple_of((1 - low) * pw, pw), 3 * pw)
    lanes_b = [pl.ds(pl.multiple_of(low * 3 * pw + lo, 128), n) for lo, n in HALVES]
    first, second = pl.ds(0, quarter), pl.ds(quarter, quarter)

    def to_sibling(f, c, r):
        return remote(prod.at[r, other, lanes[f][c]], sib.at[r, :, lanes[f][c]], sib_s.at[0], sib_r.at[c % 3, r], sibling)

    def rs(f, c, kind):
        at = lanes[f][c]
        src, dst, r = (
            (comb.at[2, first, at], diag.at[0, :, at], 1),
            (comb.at[2, second, at], diag.at[1, :, at], 2),
            (comb.at[0, first, at], rsr.at[0, first, at], 1),
            (comb.at[0, second, at], rsr.at[0, second, at], 1),
            (comb.at[1, second, at], rsr.at[1, second, at], 2),
            (comb.at[1, first, at], rsr.at[1, first, at], 2),
        )[kind]
        return remote(src, dst, rs_s.at[0], rs_r.at[c, min(kind, 2)], to_peer[r])

    def product(f, k, r, at):
        dims = (((1,), (1,)), ((), ()))
        return lax.dot_general(bufs[f][r, :, at], w[3 * f + k, :, at], dims, preferred_element_type=F32)

    def slot_in(f, r):
        @pl.when(r > (0 if f == 0 else -1))
        def _():
            at = bufs[f].at[r, other, :]
            remote(at, at, rel_s.at[0], rel_r.at[r], sibling).wait_recv()

    def silu(g):
        return g / (1.0 + jnp.exp(-g))

    every = slice(None)

    def gate_slots(f, lo, hi):
        @pl.loop(lo, hi)
        def _(r):
            slot_in(f, r)
            acc_g[r] = silu(product(f, 0, r, every))

    def up_slots(f, lo, hi):
        @pl.loop(lo, hi)
        def _(r):
            acc_u[r] = product(f, 1, r, lanes_a)

    def begin_hidden(f, lo, hi):
        @pl.loop(lo, hi)
        def _(r):
            slot_in(f, r)
            acc_g[r] = silu(product(f, 0, r, every))
            acc_u[r] = product(f, 1, r, lanes_a)

    def first_product(f, r):
        prod[r, :, lanes[f][0]] = jnp.dot(hidden[r], w[3 * f + 2, :, lanes[f][0]], preferred_element_type=F32).astype(BF16)
        to_sibling(f, 0, r).start()

    def more_hidden(f):
        @pl.loop(0, PLANE)
        def _(r):
            acc_u[r] = acc_u[r] + product(f, 1, r, lanes_b[0])

    def end_hidden(f):
        @pl.loop(0, PLANE)
        def _(k):
            r = PLANE - 1 - k
            u = acc_u[r] + product(f, 1, r, lanes_b[1])
            hidden[r] = (acc_g[r] * u).astype(BF16)
            first_product(f, r)

    def whole_hidden(f, lo, hi):
        @pl.loop(lo, hi)
        def _(r):
            slot_in(f, r)
            g = silu(product(f, 0, r, every))
            hidden[r] = (g * product(f, 1, r, every)).astype(BF16)
            first_product(f, r)

    def all_came(*pairs):
        @on_end
        def _():
            for m, slot in pairs:
                came(m, slot).wait_recv()

    def combine(f, c, r):
        at = lanes[f][c]
        to_sibling(f, c, r).wait_recv()

        @pl.loop(0, half // (2 * step))
        def _(i):
            some = pl.ds(pl.multiple_of(i * 2 * step, step), 2 * step)
            full = pl.ds(pl.multiple_of(t * half + i * 2 * step, step), 2 * step)
            comb[r - 1, some, at] = (prod[r, full, at].astype(F32) + sib[r, some, at].astype(F32)).astype(BF16)

        for kind in (None, (2,), (4,), (0, 1))[r]:
            rs(f, c, kind).start()

    def combine_all(f, c):
        for r in (3, 2, 1):
            combine(f, c, r)
        to_sibling(f, c, 0).wait_recv()

    def produce(f, c):
        at = lanes[f][c]

        @pl.loop(0, PLANE)
        def _(k):
            r = PLANE - 1 - k
            prod[r, :, at] = jnp.dot(hidden[r], w[3 * f + 2, :, at], preferred_element_type=F32).astype(BF16)
            to_sibling(f, c, r).start()

    def down(f, c):
        produce(f, c)
        combine_all(f, c)

    def finish(f, c):
        at = lanes[f][c]
        rs(f, c, 0).wait_recv()
        comb[1, first, at] = (comb[1, first, at].astype(F32) + diag[0, :, at].astype(F32)).astype(BF16)
        rs(f, c, 5).start()
        rs(f, c, 1).wait_recv()
        comb[0, second, at] = (comb[0, second, at].astype(F32) + diag[1, :, at].astype(F32)).astype(BF16)
        rs(f, c, 3).start()

    def reduced(rows_at, full, at):
        total = prod[0, full, at].astype(F32) + sib[0, rows_at, at].astype(F32)
        return total + rsr[0, rows_at, at].astype(F32) + rsr[1, rows_at, at].astype(F32)

    def out_across(c):
        at = lanes[1][c]
        return remote(here.at[:, at], fin.at[:, at], fin_s.at[0], fin_r.at[c], sibling)

    def out_store(c, k):
        at = lanes[1][c]
        return pltpu.make_async_copy((here, fin)[k].at[:, at], out_h.at[(mine, other)[k], at], store.at[0])

    def store_other(c):
        out_across(c).wait_recv()
        out_store(c, 1).start()

    def land(f, c):
        at = lanes[f][c]
        remote(rsr.at[:, :, at], rsr.at[:, :, at], rs_s.at[0], rs_r.at[c, 2], sibling).wait_recv()

        @pl.loop(0, half // (2 * step))
        def _(i):
            some = pl.ds(pl.multiple_of(i * 2 * step, step), 2 * step)
            full = pl.ds(pl.multiple_of(t * half + i * 2 * step, step), 2 * step)
            if f == 0:
                value = tokens[full, at].astype(F32) + merged[full, at].astype(F32) + 0.5 * reduced(some, full, at)
                middle[some, at] = value
                squares = value * value
                sums = sum(squares[:, k * 128:(k + 1) * 128] for k in range(sizes[f][c][1] // 128))
                ssq[some, :] = sums if c == 0 else ssq[some, :] + sums
            else:
                here[some, at] = (middle[some, at] + 0.5 * reduced(some, full, at)).astype(BF16)

        if f == 1:
            out_across(c).start()
            out_store(c, 0).start()

    def norm_first(start, count):
        @pl.loop(0, count // step)
        def _(i):
            at = pl.ds(pl.multiple_of(start + i * step, step), step)
            normed1[0, at, :] = norm_rows(tokens[at, :].astype(F32), gain1[...]).astype(BF16)

    turn(0)
    place(0)
    pl.semaphore_wait(barrier, len(targets) + mid)
    start_p1(0)
    piece_out(0, 0)
    turn(1)
    start_p1(1)
    place(1)
    piece_out(1, 0)
    for m in (3, 4):
        turn(m)
        place(m)

    @pl.when(t == 0)
    def _():
        for m in (3, 4):
            piece_out(m, 0)

    load_tokens.wait()
    load_gain1.wait()
    norm_first(t * half, half)
    for r, h in ((2, 0), (1, 1), (2, 1), (1, 0)):
        ag(0, r, h).start()
    loading(2).wait()
    start_p1(2)
    place(2)
    own_now(0)
    norm_first((1 - t) * half, half)
    own_now(1)
    pass_in(0)
    pass_out(0, 1)
    pass_in(1)
    pass_out(1, 1)
    ag_first(0)
    loading(5).wait()
    place(5)
    for m in (3, 4, 5):
        start_p1(m)
    pass_out(0, 2)
    ag_second(0)
    own_inner(2)
    begin_hidden(0, 0, 3 * mid)
    pass_out(1, 2)
    own_outer(2)
    ag_far(0)

    all_came((0, 0), (0, 1), (0, 2), (1, 0), (1, 1))
    begin_hidden(0, 3 * mid, PLANE)

    @on_end
    def _():
        for m in (3, 4, 5):
            own_inner(m)

    @on_end
    def _():
        came_part(1, 2, 0).wait_recv()

    more_hidden(0)

    @on_end
    def _():
        came_part(1, 2, 1).wait_recv()

    end_hidden(0)
    combine_all(0, 0)
    pass_in(2)
    pass_out(2, 1)

    @on_mid
    def _():
        own_inner(3)

    down(0, 1)
    finish(0, 0)
    for c in range(2, len(table[0])):
        need(0, c)
        down(0, c)
        finish(0, c - 1)
        if c == 3:
            load_merged.wait()
            load_gain2.wait()
        if c >= 3:
            land(0, c - 3)
        if c == 4:
            pass_out(2, 2)
            own_outer(3)
        if c == 5:
            pass_in(3)
            pass_out(3, 1)

            @on_mid
            def _():
                own_inner(4)

    land(0, 5)
    finish(0, 7)
    pass_in(4)

    @on_mid
    def _():
        own_inner(5)

    land(0, 6)
    land(0, 7)
    drain(ag_s.at[0], normed1.at[pl.ds(0, 3), pl.ds(0, half), :])
    drain(rel_s.at[0], normed1.at[pl.ds(0, 3), pl.ds(0, half), :])

    @pl.loop(0, half // step)
    def _(i):
        at = pl.ds(pl.multiple_of(i * step, step), step)
        full = pl.ds(pl.multiple_of(t * half + i * step, step), step)
        scale = lax.rsqrt(jnp.sum(ssq[at, :], axis=-1, keepdims=True) / width + EPS)
        normed2[0, full, :] = (middle[at, :] * scale * gain2[...]).astype(BF16)

    for r, h in ((2, 0), (1, 1), (2, 1), (1, 0)):
        ag(1, r, h).start()
    for h in range(2):
        relay(1, 0, h, t).start()
    pass_out(3, 2)
    own_outer(4)
    pass_in(5)
    pass_out(4, 1)
    ag_first(1)
    pass_out(4, 2)
    own_outer(5)
    ag_second(1)
    pass_out(5, 1)

    drain(sib_s.at[0], sib)
    drain(rs_s.at[0], comb)

    @on_mid
    def _():
        whole_hidden(1, 0, 3)

    all_came((3, 0), (3, 1), (3, 2))
    gate_slots(1, 0, 3 - 3 * mid)
    all_came((4, 0), (4, 1))
    up_slots(1, 0, 3 - 3 * mid)
    ag_far(1)
    @on_mid
    def _():
        whole_hidden(1, 3, 4)
        combine_all(1, 0)

    pass_out(5, 2)

    @on_end
    def _():
        begin_hidden(1, 3, 4)
        came_part(4, 2, 0).wait_recv()
        more_hidden(1)
        came_part(4, 2, 1).wait_recv()
        end_hidden(1)
        combine_all(1, 0)

    chunks = len(table[1])
    down(1, 1)
    finish(1, 0)
    for c in range(2, chunks - 2):
        need(1, c)
        down(1, c)
        finish(1, c - 1)
        if c >= 3:
            land(1, c - 3)
    need(1, chunks - 2)
    produce(1, chunks - 2)
    need(1, chunks - 1)
    produce(1, chunks - 1)
    combine_all(1, chunks - 2)
    combine_all(1, chunks - 1)
    finish(1, chunks - 3)
    finish(1, chunks - 2)
    land(1, chunks - 5)
    land(1, chunks - 4)
    for c in range(chunks - 4):
        store_other(c)
    finish(1, chunks - 1)
    land(1, chunks - 3)
    land(1, chunks - 2)
    land(1, chunks - 1)

    for c in range(chunks - 4, chunks):
        store_other(c)
    drain(p1_s.at[0], w.at[:, :, pl.ds(0, (PLANE - 1) * ds)])

    @on_mid
    def _():
        drain(z_s.at[0], w.at[:, :, pl.ds(0, 2 * pw)])
        drain(z_s.at[1], w.at[:, :, pl.ds(0, 3 * pw)])

    @on_end
    def _():
        drain(z_s.at[0], w.at[:, :, pl.ds(0, pw)])

    drain(ag_s.at[0], normed2.at[pl.ds(0, 3), pl.ds(0, half), :])
    drain(rel_s.at[0], normed2.at[:, pl.ds(0, half), :])
    drain(sib_s.at[0], sib)
    drain(rs_s.at[0], comb)
    drain(fin_s.at[0], here)
    pltpu.make_async_copy(tokens, tokens, store.at[0]).wait()


def plane_shards(tokens, merged, gain1, g1, u1, d1, gain2, g2, u2, d2):
    rows, width = tokens.shape
    half = rows // 2
    hid, ds = d1.shape
    q = hid // PLANE
    chunks = 2 * LINE + 1
    far = pl.BlockSpec(memory_space=pl.ANY)
    dma = lambda *s: pltpu.SemaphoreType.DMA(s)
    return pl.pallas_call(
        kernel,
        out_shape=pltpu.VMEM((rows, width), BF16),
        in_specs=[far] * 10,
        out_specs=far,
        scratch_shapes=[
            pltpu.VMEM((4, ds, hid), BF16),
            pltpu.VMEM((4, hid, ds), BF16),
            pltpu.VMEM((2, hid, ds), BF16),
            pltpu.VMEM((rows, width), BF16),
            pltpu.VMEM((rows, width), BF16),
            pltpu.VMEM((1, width), F32),
            pltpu.VMEM((1, width), F32),
            pltpu.VMEM((half, width), BF16),
            pltpu.VMEM((half, width), BF16),
            pltpu.VMEM((6, q, width), BF16),
            pltpu.VMEM((PLANE, rows, width), BF16),
            pltpu.VMEM((PLANE, rows, width), BF16),
            pltpu.VMEM((PLANE, rows, q), F32),
            pltpu.VMEM((PLANE, rows, q), F32),
            pltpu.VMEM((PLANE, rows, q), BF16),
            pltpu.VMEM((PLANE, rows, width), BF16),
            pltpu.VMEM((PLANE, half, width), BF16),
            pltpu.VMEM((PLANE - 1, half, width), BF16),
            pltpu.VMEM((2, half // 2, width), BF16),
            pltpu.VMEM((2, half, width), BF16),
            pltpu.VMEM((half, width), F32),
            pltpu.VMEM((half, 128), F32),
            dma(10), dma(1), dma(10), dma(2), dma(27),
            dma(1), dma(3, 2), dma(1), dma(PLANE),
            dma(1), dma(3, PLANE), dma(1), dma(chunks, 3),
            dma(1), dma(chunks), dma(1),
        ],
        compiler_params=pltpu.CompilerParams(
            collective_id=0, has_side_effects=True, vmem_limit_bytes=60 * 2**20
        ),
    )(tokens, merged, gain1[None], gain2[None], g1, u1, d1, g2, u2, d2)


def shards(n_fs, n_tp, *args):
    rows, width = args[0].shape
    hid, cols = args[5].shape
    fits = n_fs == PLANE * LINE and n_tp == 2 and cols % 128 == 0 and width % (512 * LINE) == 0
    fits = fits and hid % (32 * PLANE) == 0 and rows % 64 == 0
    return plane_shards(*args) if fits else gathered_shards(*args)


def solution(mesh):
    return jax.shard_map(
        functools.partial(shards, mesh.shape["fs"], mesh.shape["tp"]),
        mesh=mesh,
        in_specs=(
            P("fs", None),
            P("fs", None),
            P(),
            P("fs", "tp"),
            P("fs", "tp"),
            P("tp", "fs"),
            P(),
            P("fs", "tp"),
            P("fs", "tp"),
            P("tp", "fs"),
        ),
        out_specs=P("fs", None),
        check_vma=False,
    )
```
